32 devices in a mesh: fs: 16 (over z, y, x), tp: 2 (over core).
Axes of the slice: x: 2, y: 2, z: 4, core: 2. Of those that a mesh axis runs over, the one named last changes fastest.
Arguments:
- sequence_entries: bfloat16 [4096, 2048], P('fs', 'tp'), may hold values from -6 to 6
- former_norm_factor: float32 [2048], replicated, may hold values from 0.1 to 1.9
- conveyor_matrix: float32 [2048, 1536], P('fs', 'tp'), may hold values from -0.125 to 0.125
- conveyor_rescalers: float32 [1536], P('tp'), may hold values from 0.3 to 3
- blend_value_matrix: float32 [2048, 1536], P('fs', 'tp'), may hold values from -0.125 to 0.125
- blend_rescalers: float32 [1536], P('tp'), may hold values from 0.18 to 4.8, as said below
- blend_norm_factor: float32 [1536], P('tp'), may hold values from 0.1 to 1.9
- location_matrices: bfloat16 [24, 128, 128], P('tp'), may hold values from -0.5 to 0.5
- location_offsets: float32 [24, 128], P('tp'), may hold values from 0.1 to 1.9
- branch_emission_matrix: float32 [1536, 2048], P('tp', 'fs'), may hold values from -0.15625 to 0.15625
- emission_rescalers: float32 [2048], P('fs'), may hold values from 0.3 to 3
- latter_norm_factor: float32 [2048], replicated, may hold values from 0.1 to 1.9
- valve_matrix: float32 [2048, 5632], P('fs', 'tp'), may hold values from -0.125 to 0.125
- valve_rescalers: float32 [5632], P('tp'), may hold values from 0.3 to 3
- raising_matrix: float32 [2048, 5632], P('fs', 'tp'), may hold values from -0.125 to 0.125
- raising_rescalers: float32 [5632], P('tp'), may hold values from 0.3 to 3
- lowering_matrix: float32 [5632, 2048], P('tp', 'fs'), may hold values from -0.078125 to 0.078125
- lowering_rescalers: float32 [2048], P('fs'), may hold values from 0.3 to 3
Outputs:
- layer_out: bfloat16 [4096, 2048], P('fs', 'tp')
The draws below stay inside these ranges and needn't reach their ends.
Inputs may be any that keep to these rules, and one draw needn't show every extreme that they name: `blend_rescalers`: positive column scales.
All inputs are finite; a program needn't handle non-finite values.
Results may differ from the reference program's by a relative error of at most 0.02.
Values may be sent and summed in bfloat16 or wider, within the bound.
A program may use at most 128 MiB of HBM per device.

```python
import math
import jax
import jax.numpy as jnp
from jax import lax

MODEL_BREADTH = 2048
FILTER_BUNDLES = 24
BUNDLE_BREADTH = 64
BLEND_BREADTH = 1536
FF = 5632
BLOCK = 128
WORD_TOTALITY = 4096
N_TP = 2


def draw_blend_rescalers(key, part):
    noise_key = jax.random.fold_in(key, 11)
    place = jnp.arange(BLEND_BREADTH, dtype=jnp.float32) / max(BLEND_BREADTH - 1, 1)
    jitter = jnp.exp(jax.random.uniform(noise_key, (BLEND_BREADTH,), jnp.float32, math.log(0.6), math.log(1.6)))
    ramp = jnp.exp(math.log(0.4) + place * math.log(5.0))
    return (ramp * jitter).astype(jnp.float32)


def shard_levels(key, shape, split, least, high):
    level, own = 1.0, jax.random.fold_in(key, 6)
    for axis_at, parts in split:
        heights = jnp.exp(jax.random.uniform(jax.random.fold_in(own, axis_at), (parts,), jnp.float32, least / len(split), high / len(split)))
        level = level * jnp.repeat(heights, shape[axis_at] // parts).reshape([-1 if axis == axis_at else 1 for axis in range(len(shape))])
    return level


def scatter_about(stream_key, extent, deviation, most, shards=(), kind=jnp.bfloat16):
    array = jax.random.normal(stream_key, extent, jnp.float32) * deviation
    if len(shards) > 0:
        array = shard_levels(stream_key, extent, shards, -0.22, 0.18) * array
    return jnp.clip(array, min=-most, max=most).astype(kind)


def setup_inputs(seed: int = 0) -> dict:
    key_of = jax.random.split(jax.random.key(seed), 19)
    sequence_entries = scatter_about(key_of[0], (WORD_TOTALITY, MODEL_BREADTH), 1.0, 6.0, ((0, 16), (1, 2)))
    former_norm_factor = jnp.clip(1.0 + 0.18 * jax.random.normal(key_of[1], (MODEL_BREADTH,), jnp.float32), 0.1, 1.9)
    conveyor_matrix = scatter_about(key_of[2], (MODEL_BREADTH, BLEND_BREADTH), MODEL_BREADTH ** -0.5, 0.125, ((0, 16), (1, 2)), jnp.float32)
    conveyor_rescalers = jnp.clip(jnp.exp(math.log(3.0) - 2.3025851 * jax.random.uniform(key_of[3], (BLEND_BREADTH,), jnp.float32) ** shard_levels(key_of[3], (BLEND_BREADTH,), ((0, 2),), -0.2, 0.2)), 0.3, 3.0)
    blend_value_matrix = scatter_about(key_of[4], (MODEL_BREADTH, BLEND_BREADTH), MODEL_BREADTH ** -0.5, 0.125, ((0, 16), (1, 2)), jnp.float32)
    blend_rescalers = draw_blend_rescalers(jax.random.fold_in(key_of[18], 71), 0)
    blend_norm_factor = jnp.clip(1.0 + 0.18 * jax.random.normal(key_of[6], (BLEND_BREADTH,), jnp.float32), 0.1, 1.9)
    location_matrices = scatter_about(key_of[7], (FILTER_BUNDLES, BLOCK, BLOCK), BLOCK ** -0.5, 0.5, ((0, 2),))
    location_offsets = jnp.clip(1.0 + 0.18 * jax.random.normal(key_of[8], (FILTER_BUNDLES, BLOCK), jnp.float32), 0.1, 1.9)
    branch_emission_matrix = scatter_about(key_of[9], (BLEND_BREADTH, MODEL_BREADTH), BLEND_BREADTH ** -0.5, 0.15625, ((0, 2), (1, 16)), jnp.float32)
    emission_rescalers = jnp.clip(jnp.exp(math.log(3.0) - 2.3025851 * jax.random.uniform(key_of[10], (MODEL_BREADTH,), jnp.float32) ** shard_levels(key_of[10], (MODEL_BREADTH,), ((0, 16),), -0.2, 0.2)), 0.3, 3.0)
    latter_norm_factor = jnp.clip(1.0 + 0.18 * jax.random.normal(key_of[11], (MODEL_BREADTH,), jnp.float32), 0.1, 1.9)
    valve_matrix = scatter_about(key_of[12], (MODEL_BREADTH, FF), MODEL_BREADTH ** -0.5, 0.125, ((0, 16), (1, 2)), jnp.float32)
    valve_rescalers = jnp.clip(jnp.exp(math.log(3.0) - 2.3025851 * jax.random.uniform(key_of[13], (FF,), jnp.float32) ** shard_levels(key_of[13], (FF,), ((0, 2),), -0.2, 0.2)), 0.3, 3.0)
    raising_matrix = scatter_about(key_of[14], (MODEL_BREADTH, FF), MODEL_BREADTH ** -0.5, 0.125, ((0, 16), (1, 2)), jnp.float32)
    raising_rescalers = jnp.clip(jnp.exp(math.log(3.0) - 2.3025851 * jax.random.uniform(key_of[15], (FF,), jnp.float32) ** shard_levels(key_of[15], (FF,), ((0, 2),), -0.2, 0.2)), 0.3, 3.0)
    lowering_matrix = scatter_about(key_of[16], (FF, MODEL_BREADTH), FF ** -0.5, 0.078125, ((0, 2), (1, 16)), jnp.float32)
    lowering_rescalers = jnp.clip(jnp.exp(math.log(3.0) - 2.3025851 * jax.random.uniform(key_of[17], (MODEL_BREADTH,), jnp.float32) ** shard_levels(key_of[17], (MODEL_BREADTH,), ((0, 16),), -0.2, 0.2)), 0.3, 3.0)
    return dict(sequence_entries=sequence_entries, former_norm_factor=former_norm_factor, conveyor_matrix=conveyor_matrix, conveyor_rescalers=conveyor_rescalers, blend_value_matrix=blend_value_matrix, blend_rescalers=blend_rescalers, blend_norm_factor=blend_norm_factor, location_matrices=location_matrices, location_offsets=location_offsets, branch_emission_matrix=branch_emission_matrix, emission_rescalers=emission_rescalers, latter_norm_factor=latter_norm_factor, valve_matrix=valve_matrix, valve_rescalers=valve_rescalers, raising_matrix=raising_matrix, raising_rescalers=raising_rescalers, lowering_matrix=lowering_matrix, lowering_rescalers=lowering_rescalers)


EPS = 1e-06

def normalize(rows, gain):
    values = rows.astype(jnp.float32)
    factor = lax.rsqrt(lax.optimization_barrier(jnp.mean(values * values, axis=-1, keepdims=True)) + EPS)
    return (values * factor * gain).astype(jnp.bfloat16)

def rescaled_matmul(left, weight, scale):
    return jnp.dot(left, weight.astype(jnp.bfloat16), preferred_element_type=jnp.float32) * scale

def split_sum(left, weight, scale, groups):
    width = left.shape[1] // groups
    total = jnp.zeros((left.shape[0], weight.shape[1]), jnp.float32)
    for index in range(groups):
        part_sum = rescaled_matmul(left[:, index * width:(index + 1) * width], weight[index * width:(index + 1) * width], scale).astype(jnp.bfloat16)
        part_sum = lax.optimization_barrier(part_sum)
        total = total + part_sum.astype(jnp.float32)
    return total

def reference(sequence_entries, former_norm_factor, conveyor_matrix, conveyor_rescalers, blend_value_matrix, blend_rescalers, blend_norm_factor, location_matrices, location_offsets, branch_emission_matrix, emission_rescalers, latter_norm_factor, valve_matrix, valve_rescalers, raising_matrix, raising_rescalers, lowering_matrix, lowering_rescalers):
    standardized_source = normalize(sequence_entries, former_norm_factor)
    conveyor_current = jax.nn.gelu(rescaled_matmul(standardized_source, conveyor_matrix, conveyor_rescalers))
    signal = jax.nn.gelu(rescaled_matmul(standardized_source, blend_value_matrix, blend_rescalers))
    factor = lax.rsqrt(lax.optimization_barrier(jnp.mean(signal * signal, axis=-1, keepdims=True)) + EPS)
    signal_norm = (signal * factor * blend_norm_factor).astype(jnp.bfloat16)
    lower_mask = jnp.tril(jnp.ones((BLOCK, BLOCK), bool))
    masked = jnp.where(lower_mask[None], location_matrices.astype(jnp.float32), jnp.float32(0.0))
    signal_blocks = signal_norm.astype(jnp.float32).reshape(WORD_TOTALITY // BLOCK, BLOCK, FILTER_BUNDLES, BUNDLE_BREADTH)
    location_blended = jnp.einsum('gts,bsgd->btgd', masked, signal_blocks) + location_offsets.T[None, :, :, None]
    filtered_result = (conveyor_current * location_blended.reshape(WORD_TOTALITY, FILTER_BUNDLES * BUNDLE_BREADTH)).astype(jnp.bfloat16)
    middle = (sequence_entries.astype(jnp.float32) + split_sum(filtered_result, branch_emission_matrix, emission_rescalers, N_TP)).astype(jnp.bfloat16)
    ffn_in = normalize(middle, latter_norm_factor)
    hidden = (jax.nn.silu(rescaled_matmul(ffn_in, valve_matrix, valve_rescalers)) * rescaled_matmul(ffn_in, raising_matrix, raising_rescalers)).astype(jnp.bfloat16)
    return (middle.astype(jnp.float32) + split_sum(hidden, lowering_matrix, lowering_rescalers, N_TP)).astype(jnp.bfloat16)
```

```python
import functools

import jax
import jax.numpy as jnp
from jax import lax
from jax.experimental import pallas as pl
from jax.experimental.pallas import tpu as pltpu
from jax.sharding import PartitionSpec as P

EPS = 1e-06
MESH = pl.DeviceIdType.MESH
BF = jnp.bfloat16
F32 = jnp.float32
SCHEDULE = {
    "a0": ("PWC",),
    "a2": ("YWCb", "ZWCa",),
    "a4": ("ZWCb", "PWE", "ZWEa", "PVB", "YWEa", "FWCa",),
    "a5": ("PVA", "ZWEb",),
    "b0": ("YWCa", "ZVBa",),
    "b1": ("FWCb",),
    "b3": ("YWEb",),
    "b4": ("FWEa",),
    "c0": ("ZVAa",),
    "c1": ("YVBa",),
    "c2": ("PLA", "FWEb",),
    "c3": ("YVAa", "FVBa",),
    "d0": ("ZLAa", "PLB", "YVAb",),
    "d1": ("ZVAb",),
    "d2": ("YLAa",),
    "d4": ("FVAa",),
    "d5": ("YLBa",),
    "e0": ("ZVBb", "YLBb",),
    "e1": ("YVBb", "ZLAb", "FVAb",),
    "e2": ("FVBb",),
    "f0": ("ZLBb",),
    "f1": ("ZLBa", "YLAb",),
    "f4": ("FLAb",),
    "g0": ("FLAa",),
    "f5": ("FLBb",),
    "g4": ("FLBa",),
}
SPLITS = (16, 12, 12, 9)


def layer_kernel(
    dims,
    x_in, g1_in, cv_in, sc_in, bv_in, sb_in, gb_in, loc_in, offs_in, em_in, es_in,
    g2_in, vv_in, sv_in, rv_in, sr_in, lw_in, ls_in,
    out,
    f_cv, f_bv, f_em, f_vv, f_rv, f_lw, loc,
    g1, g2, sc_all, sb_all, gb_all, sv_all, sr_all, es, ls, offs_all,
    s_wc, s_we, s_va, s_vb, s_la, s_lb,
    wc, we, va, vb, la, lb,
    xa, xm, nrm, car, sgn, gat, hid, sq, offs, part, half, rcore, rx, rz, dx_in, dz_in,
    inl, p1s, p1r, p1l, p2s, p2r, ags, agr, sqs, sqr, rss, rsr,
):
    rows, width, chan, ff, cut, block_len, group_width, total_chan, splits = dims
    fs = lax.axis_index("fs")
    c = lax.axis_index("tp")
    x = fs % 2
    y = (fs // 2) % 2
    zl = (fs // 4) % 2
    zh = fs // 8
    ai = x + 2 * zl
    groups = chan // group_width

    def dev(dx=0, dy=0, dzl=0, dzh=0, dc=0):
        nx = 1 - x if dx else x
        ny = 1 - y if dy else y
        nzl = 1 - zl if dzl else zl
        nzh = 1 - zh if dzh else zh
        nc = 1 - c if dc else c
        return {"fs": nzh * 8 + nzl * 4 + ny * 2 + nx, "tp": nc}

    def blk(da):
        return (1 - x if da & 1 else x) + 2 * (1 - zl if da & 2 else zl)

    loads = {}

    def load(name, src, dst):
        copy = pltpu.make_async_copy(src, dst, inl.at[len(loads)])
        copy.start()
        loads[name] = copy

    load("cv", cv_in, f_cv)
    load("bv", bv_in, f_bv)
    load("x", x_in, xa.at[c, ai])
    load("em", em_in, f_em)
    load("es", es_in, es.at[0])
    load("vv", vv_in, f_vv)
    load("rv", rv_in, f_rv)
    load("ls", ls_in, ls.at[0])
    load("lw", lw_in, f_lw)
    for name, src, dst in (
        ("g1", g1_in, g1.at[0]), ("sc", sc_in, sc_all.at[0]), ("sb", sb_in, sb_all.at[0]), ("gb", gb_in, gb_all.at[0]),
        ("offs", offs_in, offs_all), ("loc", loc_in.at[pl.ds(ai * groups, groups)], loc),
        ("g2", g2_in, g2.at[0]), ("sv", sv_in, sv_all.at[0]), ("sr", sr_in, sr_all.at[0]),
    ):
        load(name, src, dst)

    peers = [dev(dx=da & 1, dzl=da & 2, dc=dc) for da in range(4) for dc in range(2) if da or dc]
    peers += [dev(dy=1), dev(dzh=1)]
    barrier = pltpu.get_barrier_semaphore()
    for peer in peers:
        pl.semaphore_signal(barrier, inc=1, device_id=peer, device_id_type=MESH)

    loads["cv"].wait()
    loads["bv"].wait()
    for q in range(4):
        s_wc[q, :, :chan] = f_cv[:, q * chan:(q + 1) * chan].astype(BF)
        s_wc[q, :, chan:] = f_bv[:, q * chan:(q + 1) * chan].astype(BF)
    loads["x"].wait()
    pl.semaphore_wait(barrier, len(peers))

    def rcopy(src, dst, ss, rs, to):
        return pltpu.make_async_remote_copy(
            src_ref=src, dst_ref=dst, send_sem=ss, recv_sem=rs, device_id=to, device_id_type=MESH
        )

    pending = []

    def go(copy):
        copy.start()
        pending.append(copy)
        return copy

    ins = (s_wc, s_we, s_va, s_vb, s_la, s_lb)
    dst = (wc, we, va, vb, la, lb)
    rowwise = (False, True, False, False, True, True)
    WC, WE, VA, VB, LA, LB = range(6)

    def cell(m):
        if rowwise[m]:
            lanes = ins[m].shape[2]
            return dst[m].at[zh, zl, :, pl.ds(pl.multiple_of((y * 2 + x) * lanes, lanes), lanes)]
        return dst[m].at[zh, zl, y, x]

    def piece(m, a, b, h):
        level = 1 - zl if h == "b" else zl
        if rowwise[m]:
            lanes = 2 * ins[m].shape[2]
            return dst[m].at[a, level, :, pl.ds(pl.multiple_of(b * lanes, lanes), lanes)]
        return dst[m].at[a, level, b]

    first = {}
    second = {}

    def phase1(m):
        local = pltpu.make_async_copy(ins[m].at[ai], cell(m), p1l.at[m])
        local.start()
        copies = {
            da: go(rcopy(ins[m].at[blk(da)], cell(m), p1s.at[m, da - 1], p1r.at[m, da - 1], dev(dx=da & 1, dzl=da & 2)))
            for da in (3, 2, 1)
        }
        first[m, "a"] = (local, copies[1])
        first[m, "b"] = (copies[2], copies[3])

    def settle(m, h):
        if (m, h) in first:
            one, two = first.pop((m, h))
            two.wait_recv()
            if h == "a":
                one.wait()
            else:
                one.wait_recv()

    def send(kind, m, h):
        i = "ZYF".index(kind) * 2 + "ab".index(h)
        if kind == "F":
            second["Z", m, h].wait_recv()
            src = piece(m, 1 - zh, y, h)
        else:
            settle(m, h)
            src = piece(m, zh, y, h)
        to = dev(dzh=1) if kind == "Z" else dev(dy=1)
        second[kind, m, h] = go(rcopy(src, src, p2s.at[m, i], p2r.at[m, i], to))

    def ready(m, kinds="YF"):
        for kind in kinds:
            for h in "ab":
                second[kind, m, h].wait_recv()

    def gather_start(buf, k):
        own = buf.at[c, ai]
        z = go(rcopy(own, own, ags.at[k, 0], agr.at[k, 0], dev(dzl=1)))
        xx = go(rcopy(own, own, ags.at[k, 1], agr.at[k, 1], dev(dx=1)))
        core = go(rcopy(own, own, ags.at[k, 2], agr.at[k, 2], dev(dc=1)))
        return [z, xx, core]

    def norm_block(buf, gain, b):
        total = jnp.zeros((rows, 1), F32)
        for h in range(2):
            v = buf[h, b].astype(F32)
            total = total + jnp.sum(v * v, axis=-1, keepdims=True)
        factor = lax.rsqrt(total / (2 * width) + EPS)
        for h in range(2):
            nrm[h, b] = (buf[h, b].astype(F32) * factor * gain[:, h * width:(h + 1) * width]).astype(BF)

    def project(w, b):
        n = w.shape[-1]
        return jnp.dot(nrm[0, b], w[0].reshape(width, n), preferred_element_type=F32) + jnp.dot(
            nrm[1, b], w[1].reshape(width, n), preferred_element_type=F32
        )

    def emit(b):
        v = gat[b]
        n = we.shape[-1]
        for h in range(2):
            for q in range(2):
                part[h, b, :, q * n:(q + 1) * n] = jnp.dot(v, we[h, q], preferred_element_type=F32).astype(BF)

    def emit_plane(b, a, p):
        n = 2 * s_la.shape[2]
        lanes = pl.ds(pl.multiple_of(p * n, n), n)
        for q in range(2):
            at = pl.ds(pl.multiple_of(q * 2 * n + p * n, n), n)
            part[a, b, :, at] = (
                jnp.dot(hid[b, :, :cut], la[a, q, :, lanes], preferred_element_type=F32)
                + jnp.dot(hid[b, :, cut:], lb[a, q, :, lanes], preferred_element_type=F32)
            ).astype(BF)

    order = (3, 1, 2, 0)

    def scatter_cores(k):
        cores = {
            da: rcopy(part.at[1 - c, blk(da)], rcore.at[k, blk(da)], rss.at[k, i], rsr.at[k, i], dev(dc=1))
            for i, da in enumerate(order)
        }
        return cores

    def scatter_links(k):
        cutoff = splits[2 + k]
        rest = rows - cutoff
        top, bottom = pl.ds(0, cutoff), pl.ds(cutoff, rest)
        zb, xb, db = blk(2), blk(1), blk(3)
        links = {
            "dx": rcopy(half.at[k, db, top], dx_in.at[k, top], rss.at[k, 4], rsr.at[k, 4], dev(dx=1)),
            "x0": rcopy(half.at[k, xb, top], rx.at[k, top], rss.at[k, 7], rsr.at[k, 7], dev(dx=1)),
            "z1": rcopy(half.at[k, zb, top], rz.at[k, top], rss.at[k, 8], rsr.at[k, 8], dev(dzl=1)),
        }
        if rest:
            links["dz"] = rcopy(
                half.at[k, db, bottom], dz_in.at[k, bottom], rss.at[k, 5], rsr.at[k, 5], dev(dzl=1)
            )
            links["z0"] = rcopy(half.at[k, zb, bottom], rz.at[k, bottom], rss.at[k, 6], rsr.at[k, 6], dev(dzl=1))
            links["x1"] = rcopy(half.at[k, xb, bottom], rx.at[k, bottom], rss.at[k, 9], rsr.at[k, 9], dev(dx=1))
        pending.extend(links.values())
        return links, top, bottom

    def scatter_first(k, cores, plan):
        links, top, bottom = plan

        def combine(da):
            b = blk(da)
            cores[da].wait_recv()
            half[k, b] = (part[c, b].astype(F32) + rcore[k, b].astype(F32)).astype(BF)

        combine(3)
        links["dx"].start()
        if "dz" in links:
            links["dz"].start()
        combine(1)
        links["x0"].start()
        combine(2)
        if "z0" in links:
            links["z0"].start()

    def scatter_second(k, cores, plan, tag):
        links, top, bottom = plan
        zb, xb = blk(2), blk(1)
        slot_of(tag + "0")
        links["dx"].wait_recv()
        half[k, zb, top] = (half[k, zb, top].astype(F32) + dx_in[k, top].astype(F32)).astype(BF)
        links["z1"].start()
        if "dz" in links:
            links["dz"].wait_recv()
            half[k, xb, bottom] = (half[k, xb, bottom].astype(F32) + dz_in[k, bottom].astype(F32)).astype(BF)
            links["x1"].start()
        slot_of(tag + "1")
        cores[0].wait_recv()
        for da in order:
            cores[da].wait_send()
        own = part[c, ai].astype(F32) + rcore[k, ai].astype(F32)
        for name in ("x0", "z0", "z1", "x1"):
            if name in links:
                links[name].wait_recv()
        return own + rz[k].astype(F32) + rx[k].astype(F32)

    def pick(ref, n, lo, hi):
        value = ref[:, lo:hi]
        for k in range(1, 4):
            value = jnp.where(ai == k, ref[:, k * n + lo:k * n + hi], value)
        return value

    names = {"WC": WC, "WE": WE, "VA": VA, "VB": VB, "LA": LA, "LB": LB}

    def slot_of(name):
        for step in SCHEDULE.get(name, ()):
            m = names[step[1:3]]
            if step[0] == "P":
                phase1(m)
            else:
                send(step[0], m, step[3])

    def gather(buf, k, gain, st, tag, early, late):
        z, xx, core = st
        cutoff = splits[k]
        z.wait_recv()
        zb = buf.at[c, blk(2)]
        zbt = buf.at[c, blk(2), pl.ds(0, cutoff)]
        diag = [go(rcopy(zbt, zbt, ags.at[k, 3], agr.at[k, 3], dev(dx=1)))]
        zcore = go(rcopy(zb, zb, ags.at[k, 4], agr.at[k, 4], dev(dc=1)))
        slot_of(tag + "0")
        xx.wait_recv()
        xb = buf.at[c, blk(1)]
        if cutoff < rows:
            xbb = buf.at[c, blk(1), pl.ds(cutoff, rows - cutoff)]
            diag.append(go(rcopy(xbb, xbb, ags.at[k, 5], agr.at[k, 5], dev(dzl=1))))
        xcore = go(rcopy(xb, xb, ags.at[k, 6], agr.at[k, 6], dev(dc=1)))
        slot_of(tag + "1")
        core.wait_recv()
        norm_block(buf, gain, blk(0))
        slot_of(tag + "2")
        zcore.wait_recv()
        norm_block(buf, gain, blk(2))
        slot_of(tag + "3")
        xcore.wait_recv()
        norm_block(buf, gain, blk(1))
        slot_of(tag + "4")
        early()
        for copy in diag:
            copy.wait_recv()
        db = buf.at[c, blk(3)]
        dcore = go(rcopy(db, db, ags.at[k, 7], agr.at[k, 7], dev(dc=1)))
        slot_of(tag + "5")
        dcore.wait_recv()
        norm_block(buf, gain, blk(3))
        slot_of(tag + "6")
        late()

    slot_of("a0")
    st1 = gather_start(xa, 0)
    slot_of("a1")
    loads["em"].wait()
    loads["es"].wait()
    for q in range(4):
        s_we[q] = (f_em[q * chan:(q + 1) * chan] * es[...]).astype(BF)
    slot_of("a2")
    loads["vv"].wait()
    loads["rv"].wait()
    for q in range(4):
        base = q * ff
        s_va[q, :, :cut] = f_vv[:, base:base + cut].astype(BF)
        s_va[q, :, cut:] = f_rv[:, base:base + cut].astype(BF)
    slot_of("a3")
    for q in range(4):
        base = q * ff
        s_vb[q, :, :ff - cut] = f_vv[:, base + cut:base + ff].astype(BF)
        s_vb[q, :, ff - cut:] = f_rv[:, base + cut:base + ff].astype(BF)
    slot_of("a4")
    loads["ls"].wait()
    loads["lw"].wait()
    for q in range(4):
        base = q * ff
        s_la[q] = (f_lw[base:base + cut] * ls[...]).astype(BF)
        s_lb[q] = (f_lw[base + cut:base + ff] * ls[...]).astype(BF)
    slot_of("a5")
    for name in ("g1", "sc", "sb", "gb", "offs", "loc", "g2", "sv", "sr"):
        loads[name].wait()
    head = lax.broadcasted_iota(jnp.int32, (offs_all.shape[0], chan), 0)
    lane = lax.broadcasted_iota(jnp.int32, (offs_all.shape[0], chan), 1)
    chosen = (lane >= (head - ai * groups) * group_width) & (lane < (head - ai * groups + 1) * group_width)
    offs[...] = lax.dot_general(
        offs_all[...], chosen.astype(F32), (((0,), (0,)), ((), ())),
        precision=lax.Precision.HIGHEST, preferred_element_type=F32,
    )
    slot = ai * 2 + c

    def first_projection(da):
        b = blk(da)
        sc, sb, gb = (pick(v, chan, 0, chan) for v in (sc_all, sb_all, gb_all))
        both = project(wc, b)
        car[b] = jax.nn.gelu(both[:, :chan] * sc)
        signal = jax.nn.gelu(both[:, chan:] * sb)
        sgn[b] = (signal * gb).astype(BF)
        sq[slot, b] = lax.dot_general(
            jnp.ones((8, chan), F32), signal * signal, (((1,), (1,)), ((), ())),
            precision=lax.Precision.HIGHEST, preferred_element_type=F32,
        )

    def first_early():
        ready(WC)
        slot_of("c0")
        for i, da in enumerate((0, 2, 1)):
            first_projection(da)
            slot_of(f"c{i + 1}")

    def first_late():
        first_projection(3)
        slot_of("c4")

    gather(xa, 0, g1, st1, "b", first_early, first_late)
    squares = []
    for da in range(4):
        for dc in range(2):
            if da or dc:
                i = da * 2 + dc - 1
                squares.append(
                    go(rcopy(sq.at[slot], sq.at[slot], sqs.at[i], sqr.at[i], dev(dx=da & 1, dzl=da & 2, dc=dc)))
                )
    slot_of("d0")
    for copy in squares:
        copy.wait_recv()
    slot_of("d1")
    lower = lax.broadcasted_iota(jnp.int32, (block_len, block_len), 0) >= lax.broadcasted_iota(
        jnp.int32, (block_len, block_len), 1
    )
    lane = lax.broadcasted_iota(jnp.int32, (block_len, chan), 1)
    cores1 = scatter_cores(0)
    ready(WE)
    for i, da in enumerate(order):
        b = blk(da)
        total = sq[0, b]
        for j in range(1, 8):
            total = total + sq[j, b]
        factor = lax.rsqrt(total / total_chan + EPS)
        for s in range(rows // block_len):
            span = slice(s * block_len, (s + 1) * block_len)
            values = sgn[b, span]
            mixed = jnp.zeros((block_len, chan), F32)
            for g in range(groups):
                mat = jnp.where(lower, loc[g].astype(F32), 0.0) * factor[0:1, span]
                one = jnp.dot(mat.astype(BF), values, preferred_element_type=F32)
                inside = (lane >= g * group_width) & (lane < (g + 1) * group_width)
                mixed = jnp.where(inside, one, mixed)
            gat[b, span] = (car[b, span] * (mixed + offs[...])).astype(BF)
        emit(b)
        cores1[da].start()
        slot_of(f"d{i + 2}")
    plan1 = scatter_links(0)
    scatter_first(0, cores1, plan1)
    summed = scatter_second(0, cores1, plan1, "e")
    xm[c, ai] = (xa[c, ai].astype(F32) + summed).astype(BF)
    st2 = gather_start(xm, 1)
    slot_of("e2")

    def up_projection(w, lo, hi, da):
        b = blk(da)
        sv, sr = (pick(v, ff, lo, hi) for v in (sv_all, sr_all))
        both = project(w, b)
        gate = both[:, :hi - lo] * sv
        up = both[:, hi - lo:] * sr
        hid[b, :, lo:hi] = (jax.nn.silu(gate) * up).astype(BF)

    ups = ((VA, va, 0, cut, "g"), (VB, vb, cut, ff, "h"))

    def second_early():
        for m, w, lo, hi, tag in ups:
            ready(m)
            slot_of(tag + "0")
            for i, da in enumerate((0, 2, 1)):
                up_projection(w, lo, hi, da)
                slot_of(f"{tag}{i + 1}")

    def second_late():
        for m, w, lo, hi, tag in ups:
            up_projection(w, lo, hi, 3)
            slot_of(tag + "4")

    gather(xm, 1, g2, st2, "f", second_early, second_late)
    cores2 = scatter_cores(1)
    plan2 = scatter_links(1)
    for far in range(2):
        a = 1 - zh if far else zh
        for off in range(2):
            p = 1 - y if off else y
            if off:
                for m in (LA, LB):
                    ready(m, "YF"[far])
            for i, da in enumerate(order):
                emit_plane(blk(da), a, p)
                if off:

                    @pl.when(c != a)
                    def _():
                        cores2[da].start()

            if not far:
                slot_of(f"i{off}")

        @pl.when(c == a)
        def _():
            scatter_first(1, cores2, plan2)

    summed = scatter_second(1, cores2, plan2, "j")
    out[...] = (xm[c, ai].astype(F32) + summed).astype(BF)
    for copy in pending:
        copy.wait_send()


def on_device_fused(
    sequence_entries, former_norm_factor, conveyor_matrix, conveyor_rescalers,
    blend_value_matrix, blend_rescalers, blend_norm_factor, location_matrices,
    location_offsets, branch_emission_matrix, emission_rescalers, latter_norm_factor,
    valve_matrix, valve_rescalers, raising_matrix, raising_rescalers,
    lowering_matrix, lowering_rescalers,
):
    parts = 4
    rows, width = sequence_entries.shape
    depth, chans = conveyor_matrix.shape
    chan = chans // parts
    hidden = valve_matrix.shape[1]
    ff = hidden // parts
    cut = (ff // 2 + 127) // 128 * 128
    heads = location_matrices.shape[0]
    groups = heads // parts
    block_len = location_matrices.shape[1]
    group_width = chan // groups
    total_chan = chans * lax.axis_size("tp")
    cols = branch_emission_matrix.shape[1]
    args = (
        sequence_entries, former_norm_factor, conveyor_matrix, conveyor_rescalers,
        blend_value_matrix, blend_rescalers, blend_norm_factor, location_matrices,
        location_offsets, branch_emission_matrix, emission_rescalers, latter_norm_factor,
        valve_matrix, valve_rescalers, raising_matrix, raising_rescalers,
        lowering_matrix, lowering_rescalers,
    )
    vm = pltpu.VMEM
    dma = pltpu.SemaphoreType.DMA
    cube = (2, 2, 2, 2, depth)
    scratch = [
        vm((depth, chans), F32), vm((depth, chans), F32), vm((chans, cols), F32),
        vm((depth, hidden), F32), vm((depth, hidden), F32), vm((hidden, cols), F32),
        vm((groups, block_len, block_len), BF),
        vm((1, 2 * width), F32), vm((1, 2 * width), F32), vm((1, chans), F32), vm((1, chans), F32),
        vm((1, chans), F32), vm((1, hidden), F32), vm((1, hidden), F32), vm((1, cols), F32),
        vm((1, cols), F32), vm((heads, block_len), F32),
        vm((parts, depth, 2 * chan), BF), vm((parts, chan, cols), BF),
        vm((parts, depth, 2 * cut), BF), vm((parts, depth, 2 * (ff - cut)), BF),
        vm((parts, cut, cols), BF), vm((parts, ff - cut, cols), BF),
        vm(cube + (2 * chan,), BF), vm((2, 2, chan, 4 * cols), BF),
        vm(cube + (2 * cut,), BF), vm(cube + (2 * (ff - cut),), BF),
        vm((2, 2, cut, 4 * cols), BF), vm((2, 2, ff - cut, 4 * cols), BF),
        vm((2, 4, rows, width), BF), vm((2, 4, rows, width), BF), vm((2, 4, rows, width), BF),
        vm((4, rows, chan), F32), vm((4, rows, chan), BF), vm((4, rows, chan), BF),
        vm((4, rows, ff), BF), vm((8, 4, 8, rows), F32), vm((block_len, chan), F32),
        vm((2, 4, rows, width), BF), vm((2, 4, rows, width), BF), vm((2, 4, rows, width), BF),
        vm((2, rows, width), BF), vm((2, rows, width), BF),
        vm((2, rows, width), BF), vm((2, rows, width), BF),
        dma((18,)), dma((6, 3)), dma((6, 3)), dma((6,)), dma((6, 6)), dma((6, 6)),
        dma((2, 8)), dma((2, 8)), dma((7,)), dma((7,)), dma((2, 10)), dma((2, 10)),
    ]
    splits = tuple(rows * part // 16 for part in SPLITS)
    dims = (rows, width, chan, ff, cut, block_len, group_width, total_chan, splits)
    return pl.pallas_call(
        functools.partial(layer_kernel, dims),
        out_shape=jax.ShapeDtypeStruct((rows, width), BF),
        in_specs=[pl.BlockSpec(memory_space=pl.ANY)] * len(args),
        out_specs=pl.BlockSpec(memory_space=pltpu.VMEM),
        scratch_shapes=scratch,
        compiler_params=pltpu.CompilerParams(
            collective_id=0, has_side_effects=True, vmem_limit_bytes=66000000
        ),
    )(*args)


def normalize(rows, gain):
    values = rows.astype(jnp.float32)
    factor = lax.rsqrt(jnp.mean(values * values, axis=-1, keepdims=True) + EPS)
    return (values * factor * gain).astype(jnp.bfloat16)


def elementwise_plus(left_rows, pieces):
    return (
        jnp.dot(left_rows, pieces[0], preferred_element_type=jnp.float32),
        jnp.dot(left_rows, pieces[1], preferred_element_type=jnp.float32),
    )


def project_cols(left_rows, scales, piece):
    return jnp.dot(left_rows, piece, preferred_element_type=jnp.float32) * scales


def on_device(
    sequence_entries,
    former_norm_factor,
    conveyor_matrix,
    conveyor_rescalers,
    blend_value_matrix,
    blend_rescalers,
    blend_norm_factor,
    location_matrices,
    location_offsets,
    branch_emission_matrix,
    emission_rescalers,
    latter_norm_factor,
    valve_matrix,
    valve_rescalers,
    raising_matrix,
    raising_rescalers,
    lowering_matrix,
    lowering_rescalers,
):
    out_scales, down_scales = (
        lax.all_gather(emission_rescalers, "fs", axis=0, tiled=True),
        lax.all_gather(lowering_rescalers, "fs", axis=0, tiled=True),
    )
    full_rows = lax.all_gather(sequence_entries, "tp", axis=1, tiled=True)
    own_width = sequence_entries.shape[1]
    own_start = lax.axis_index("tp") * own_width
    standardized_source = normalize(full_rows, former_norm_factor)
    conveyor_prior, stream_prior = elementwise_plus(
        standardized_source,
        (
            lax.all_gather(conveyor_matrix.astype(jnp.bfloat16), "fs", axis=0, tiled=True),
            lax.all_gather(blend_value_matrix.astype(jnp.bfloat16), "fs", axis=0, tiled=True),
        ),
    )
    conveyor_current = jax.nn.gelu(conveyor_prior * conveyor_rescalers)
    signal = jax.nn.gelu(stream_prior * blend_rescalers)
    total_sq = lax.psum(jnp.sum(signal * signal, axis=1), "tp")
    channels = signal.shape[1] * lax.axis_size("tp")
    signal_norm = (
        signal * lax.rsqrt(total_sq / channels + EPS)[:, None] * blend_norm_factor
    ).astype(jnp.bfloat16)
    local_groups = location_matrices.shape[0]
    block_len = location_matrices.shape[1]
    group_width = signal.shape[1] // local_groups
    lower_mask = jnp.tril(jnp.ones((block_len, block_len), bool))
    masked = jnp.where(lower_mask[None], location_matrices, jnp.zeros((), jnp.bfloat16))
    signal_blocks = signal_norm.reshape(-1, block_len, local_groups, group_width)
    location_blended = jnp.einsum(
        "gts,bsgd->btgd", masked, signal_blocks, preferred_element_type=jnp.float32
    )
    location_blended = location_blended + location_offsets.T[None, :, :, None]
    filtered_result = (conveyor_current * location_blended.reshape(conveyor_current.shape)).astype(
        jnp.bfloat16
    )
    mixer_terms = project_cols(
        filtered_result,
        out_scales,
        lax.all_gather(branch_emission_matrix.astype(jnp.bfloat16), "fs", axis=1, tiled=True),
    )
    summed = lax.psum(mixer_terms.astype(jnp.bfloat16), "tp").astype(jnp.float32)
    mid_rows = (full_rows.astype(jnp.float32) + summed).astype(jnp.bfloat16)
    mid_own = lax.dynamic_slice_in_dim(mid_rows, own_start, own_width, 1)
    ffn_in = normalize(mid_rows, latter_norm_factor)
    gate_half = valve_matrix.astype(jnp.bfloat16)
    up_half = raising_matrix.astype(jnp.bfloat16)
    whole_gate, whole_up = (
        lax.all_gather(gate_half, "fs", axis=0, tiled=True),
        lax.all_gather(up_half, "fs", axis=0, tiled=True),
    )
    pre_gate = jnp.dot(ffn_in, whole_gate, preferred_element_type=jnp.float32)
    pre_up = jnp.dot(ffn_in, whole_up, preferred_element_type=jnp.float32)
    hidden = (jax.nn.silu(pre_gate * valve_rescalers) * (pre_up * raising_rescalers)).astype(
        jnp.bfloat16
    )
    ffn_terms = project_cols(
        hidden,
        down_scales,
        lax.all_gather(lowering_matrix.astype(jnp.bfloat16), "fs", axis=1, tiled=True),
    )
    ffn_share = lax.psum_scatter(
        ffn_terms.astype(jnp.bfloat16), "tp", scatter_dimension=1, tiled=True
    ).astype(jnp.float32)
    return (mid_own.astype(jnp.float32) + ffn_share).astype(jnp.bfloat16)


def solution(mesh):
    sizes = dict(mesh.shape)
    fused = sizes["tp"] == 2 and sizes["fs"] == 16
    return jax.shard_map(
        on_device_fused if fused else on_device,
        mesh=mesh,
        in_specs=(
            P("fs", "tp"),
            P(),
            P("fs", "tp"),
            P("tp"),
            P("fs", "tp"),
            P("tp"),
            P("tp"),
            P("tp", None, None),
            P("tp", None),
            P("tp", "fs"),
            P("fs"),
            P(),
            P("fs", "tp"),
            P("tp"),
            P("fs", "tp"),
            P("tp"),
            P("tp", "fs"),
            P("fs"),
        ),
        out_specs=P("fs", "tp"),
        check_vma=False,
    )
```

```python
import functools

import jax
import jax.numpy as jnp
from jax import lax
from jax.experimental import pallas as pl
from jax.experimental.pallas import tpu as pltpu
from jax.sharding import PartitionSpec as P

EPS = 1e-06
MESH = pl.DeviceIdType.MESH
BF = jnp.bfloat16
F32 = jnp.float32
SCHEDULE = {
    "a0": ("PWC",),
    "a4": ("PVA", "LWC", "HWC", "XWC",),
    "a5": ("PVB", "YVAa", "UWC",),
    "b0": ("PWE", "ZVAb",),
    "b1": ("MWC", "VWC", "ZVAa",),
    "b2": ("XWE", "YVBa", "HWE",),
    "b3": ("YVAb", "PLA", "LWE",),
    "b4": ("QWC", "FVAb",),
    "b5": ("FVAa",),
    "c0": ("ZLAb", "VWE",),
    "c1": ("YLAa", "MWE", "ZVBa",),
    "c2": ("UWE",),
    "d0": ("ZVBb", "YVBb", "PLB",),
    "d1": ("YLBa", "QWE",),
    "e1": ("FVBa",),
    "e2": ("ZLBa", "FLAb", "YLAb", "FVBb",),
    "f0": ("ZLBb",),
    "g0": ("FLBa",),
    "g2": ("ZLAa",),
    "g3": ("YLBb",),
    "f6": ("FLBb",),
    "i1": ("FLAa",),
}
SPLITS = (9, 9)


def layer_kernel(
    dims,
    x_in, g1_in, cv_in, sc_in, bv_in, sb_in, gb_in, loc_in, offs_in, em_in, es_in,
    g2_in, vv_in, sv_in, rv_in, sr_in, lw_in, ls_in,
    out,
    f_cv, f_bv, f_em, f_vv, f_rv, f_lw, loc,
    g1, g2, sc_all, sb_all, gb_all, sv_all, sr_all, es, ls, offs_all,
    s_wc, s_we, s_va, s_vb, s_la, s_lb,
    wc, we, va, vb, la, lb,
    xa, xm, nrm, car, sgn, gat, hid, sq, offs, part, half, rcore, rx, rz, dx_in, dz_in, mhalf, mcore, ry,
    inl, p1s, p1r, p1l, p2s, p2r, ags, agr, sqs, sqr, rss, rsr, ws, wr, xs, xr, ms, mr,
):
    rows, width, chan, ff, cut, block_len, group_width, total_chan, splits = dims
    fs = lax.axis_index("fs")
    c = lax.axis_index("tp")
    x = fs % 2
    y = (fs // 2) % 2
    zl = (fs // 4) % 2
    zh = fs // 8
    ai = x + 2 * zl
    groups = chan // group_width

    def dev(dx=0, dy=0, dzl=0, dzh=0, dc=0):
        nx = 1 - x if dx else x
        ny = 1 - y if dy else y
        nzl = 1 - zl if dzl else zl
        nzh = 1 - zh if dzh else zh
        nc = 1 - c if dc else c
        return {"fs": nzh * 8 + nzl * 4 + ny * 2 + nx, "tp": nc}

    def blk(da):
        return (1 - x if da & 1 else x) + 2 * (1 - zl if da & 2 else zl)

    loads = {}

    def load(name, src, dst):
        copy = pltpu.make_async_copy(src, dst, inl.at[len(loads)])
        copy.start()
        loads[name] = copy

    load("cv", cv_in, f_cv)
    load("bv", bv_in, f_bv)
    load("x", x_in, xa.at[c, y])
    load("em", em_in, f_em)
    load("es", es_in, es.at[0])
    load("vv", vv_in, f_vv)
    load("rv", rv_in, f_rv)
    load("ls", ls_in, ls.at[0])
    load("lw", lw_in, f_lw)
    for name, src, dst in (
        ("g1", g1_in, g1.at[0]), ("sc", sc_in, sc_all.at[0]), ("sb", sb_in, sb_all.at[0]), ("gb", gb_in, gb_all.at[0]),
        ("offs", offs_in, offs_all), ("loc", loc_in.at[pl.ds(y * groups, groups)], loc),
        ("g2", g2_in, g2.at[0]), ("sv", sv_in, sv_all.at[0]), ("sr", sr_in, sr_all.at[0]),
    ):
        load(name, src, dst)

    peers = [dev(dx=da & 1, dzl=da & 2, dc=dc) for da in range(4) for dc in range(2) if da or dc]
    peers += [dev(dy=1), dev(dy=1, dc=1), dev(dzh=1)]
    barrier = pltpu.get_barrier_semaphore()
    for peer in peers:
        pl.semaphore_signal(barrier, inc=1, device_id=peer, device_id_type=MESH)

    loads["cv"].wait()
    loads["bv"].wait()
    for q in range(2):
        s_wc[q, :, :chan] = f_cv[:, q * chan:(q + 1) * chan].astype(BF)
        s_wc[q, :, chan:] = f_bv[:, q * chan:(q + 1) * chan].astype(BF)
    loads["x"].wait()
    pl.semaphore_wait(barrier, len(peers))

    def rcopy(src, dst, ss, rs, to):
        return pltpu.make_async_remote_copy(
            src_ref=src, dst_ref=dst, send_sem=ss, recv_sem=rs, device_id=to, device_id_type=MESH
        )

    pending = []

    def go(copy):
        copy.start()
        pending.append(copy)
        return copy

    ins = (s_wc, s_we, s_va, s_vb, s_la, s_lb)
    dst = (wc, we, va, vb, la, lb)
    rowwise = (False, True, False, False, True, True)
    WC, WE, VA, VB, LA, LB = range(6)

    def cell(m):
        if m == WE:
            lanes = ins[m].shape[2]
            return we.at[zh, zl, x, :, pl.ds(pl.multiple_of(y * lanes, lanes), lanes)]
        if rowwise[m]:
            lanes = ins[m].shape[2]
            return dst[m].at[zh, zl, :, pl.ds(pl.multiple_of((y * 2 + x) * lanes, lanes), lanes)]
        return dst[m].at[zh, zl, y, x]

    def level(m, a, b):
        return we.at[a, b, x] if m == WE else wc.at[a, b, :, x]

    first = {}
    moved = {}
    landed = set()

    def mixer_send(kind, m):
        i = "PLHXMUVQ".index(kind)

        def move(src, to, into=None):
            moved[kind, m] = go(rcopy(src, src if into is None else into, ws.at[m, i], wr.at[m, i], to))

        if kind == "P":
            first[m] = pltpu.make_async_copy(ins[m].at[y], cell(m), p1l.at[m])
            first[m].start()
            move(ins[m].at[1 - y], dev(dy=1), cell(m))
            return
        if m in first:
            first.pop(m).wait()
            moved["P", m].wait_recv()
        source = {"U": "L", "V": "H", "M": "H", "Q": "M"}.get(kind)
        if source and (source, m) not in landed:
            landed.add((source, m))
            moved[source, m].wait_recv()
        far, other = kind in "MVQ", kind in "UQ"
        src = level(m, 1 - zh if far else zh, 1 - zl if other else zl)
        move(src, dev(dzh=1) if kind == "H" else dev(dzl=1) if kind in "LM" else dev(dx=1))

    def mixer_ready(m):
        for kind in "XUVQ":
            moved[kind, m].wait_recv()

    def piece(m, a, b, h):
        level = 1 - zl if h == "b" else zl
        if rowwise[m]:
            lanes = 2 * ins[m].shape[2]
            return dst[m].at[a, level, :, pl.ds(pl.multiple_of(b * lanes, lanes), lanes)]
        return dst[m].at[a, level, b]

    second = {}

    def phase1(m):
        local = pltpu.make_async_copy(ins[m].at[ai], cell(m), p1l.at[m])
        local.start()
        copies = {
            da: go(rcopy(ins[m].at[blk(da)], cell(m), p1s.at[m, da - 1], p1r.at[m, da - 1], dev(dx=da & 1, dzl=da & 2)))
            for da in (3, 2, 1)
        }
        first[m, "a"] = (local, copies[1])
        first[m, "b"] = (copies[2], copies[3])

    def settle(m, h):
        if (m, h) in first:
            one, two = first.pop((m, h))
            two.wait_recv()
            if h == "a":
                one.wait()
            else:
                one.wait_recv()

    def send(kind, m, h):
        i = "ZYF".index(kind) * 2 + "ab".index(h)
        if kind == "F":
            second["Z", m, h].wait_recv()
            src = piece(m, 1 - zh, y, h)
        else:
            settle(m, h)
            src = piece(m, zh, y, h)
        to = dev(dzh=1) if kind == "Z" else dev(dy=1)
        second[kind, m, h] = go(rcopy(src, src, p2s.at[m, i], p2r.at[m, i], to))

    def ready(m, kinds="YF"):
        for kind in kinds:
            for h in "ab":
                second[kind, m, h].wait_recv()

    def gather_start(buf, k):
        own = buf.at[c, ai]
        z = go(rcopy(own, own, ags.at[k, 0], agr.at[k, 0], dev(dzl=1)))
        xx = go(rcopy(own, own, ags.at[k, 1], agr.at[k, 1], dev(dx=1)))
        core = go(rcopy(own, own, ags.at[k, 2], agr.at[k, 2], dev(dc=1)))
        return [z, xx, core]

    def norm_block(buf, gain, b):
        total = jnp.zeros((rows, 1), F32)
        for h in range(2):
            v = buf[h, b].astype(F32)
            total = total + jnp.sum(v * v, axis=-1, keepdims=True)
        factor = lax.rsqrt(total / (2 * width) + EPS)
        for h in range(2):
            nrm[h, b] = (buf[h, b].astype(F32) * factor * gain[:, h * width:(h + 1) * width]).astype(BF)

    def project(w, b):
        n = w.shape[-1]
        return jnp.dot(nrm[0, b], w[0].reshape(width, n), preferred_element_type=F32) + jnp.dot(
            nrm[1, b], w[1].reshape(width, n), preferred_element_type=F32
        )

    def emit(b):
        v = gat[b]
        n = s_we.shape[-1]
        for h in range(2):
            for q in range(2):
                for xx in range(2):
                    both = jnp.dot(v, we[h, q, xx], preferred_element_type=F32).astype(BF)
                    for yy in range(2):
                        at = ((q * 2 + yy) * 2 + xx) * n
                        part[h, b, :, at:at + n] = both[:, yy * n:(yy + 1) * n]

    def emit_plane(b, a, p):
        n = 2 * s_la.shape[2]
        lanes = pl.ds(pl.multiple_of(p * n, n), n)
        for q in range(2):
            at = pl.ds(pl.multiple_of(q * 2 * n + p * n, n), n)
            part[a, b, :, at] = (
                jnp.dot(hid[b, :, :cut], la[a, q, :, lanes], preferred_element_type=F32)
                + jnp.dot(hid[b, :, cut:], lb[a, q, :, lanes], preferred_element_type=F32)
            ).astype(BF)

    order = (3, 1, 2, 0)

    def scatter_cores(k):
        cores = {
            da: rcopy(part.at[1 - c, blk(da)], rcore.at[k, blk(da)], rss.at[k, i], rsr.at[k, i], dev(dc=1))
            for i, da in enumerate(order)
        }
        return cores

    def scatter_links(k):
        cutoff = splits[1 + k]
        rest = rows - cutoff
        top, bottom = pl.ds(0, cutoff), pl.ds(cutoff, rest)
        zb, xb, db = blk(2), blk(1), blk(3)
        links = {
            "dx": rcopy(half.at[k, db, top], dx_in.at[k, top], rss.at[k, 4], rsr.at[k, 4], dev(dx=1)),
            "x0": rcopy(half.at[k, xb, top], rx.at[k, top], rss.at[k, 7], rsr.at[k, 7], dev(dx=1)),
            "z1": rcopy(half.at[k, zb, top], rz.at[k, top], rss.at[k, 8], rsr.at[k, 8], dev(dzl=1)),
        }
        if rest:
            links["dz"] = rcopy(
                half.at[k, db, bottom], dz_in.at[k, bottom], rss.at[k, 5], rsr.at[k, 5], dev(dzl=1)
            )
            links["z0"] = rcopy(half.at[k, zb, bottom], rz.at[k, bottom], rss.at[k, 6], rsr.at[k, 6], dev(dzl=1))
            links["x1"] = rcopy(half.at[k, xb, bottom], rx.at[k, bottom], rss.at[k, 9], rsr.at[k, 9], dev(dx=1))
        pending.extend(links.values())
        return links, top, bottom

    def scatter_first(k, cores, plan):
        links, top, bottom = plan

        def combine(da):
            b = blk(da)
            cores[da].wait_recv()
            half[k, b] = (part[c, b].astype(F32) + rcore[k, b].astype(F32)).astype(BF)

        combine(3)
        links["dx"].start()
        if "dz" in links:
            links["dz"].start()
        combine(1)
        links["x0"].start()
        combine(2)
        if "z0" in links:
            links["z0"].start()

    def scatter_second(k, cores, plan, tag):
        links, top, bottom = plan
        zb, xb = blk(2), blk(1)
        slot_of(tag + "0")
        links["dx"].wait_recv()
        half[k, zb, top] = (half[k, zb, top].astype(F32) + dx_in[k, top].astype(F32)).astype(BF)
        links["z1"].start()
        if "dz" in links:
            links["dz"].wait_recv()
            half[k, xb, bottom] = (half[k, xb, bottom].astype(F32) + dz_in[k, bottom].astype(F32)).astype(BF)
            links["x1"].start()
        slot_of(tag + "1")
        cores[0].wait_recv()
        for da in order:
            cores[da].wait_send()
        own = part[c, ai].astype(F32) + rcore[k, ai].astype(F32)
        for name in ("x0", "z0", "z1", "x1"):
            if name in links:
                links[name].wait_recv()
        return own + rz[k].astype(F32) + rx[k].astype(F32)

    def pick(ref, n, lo, hi):
        value = ref[:, lo:hi]
        for k in range(1, ref.shape[1] // n):
            value = jnp.where((ai if ref.shape[1] // n == 4 else y) == k, ref[:, k * n + lo:k * n + hi], value)
        return value

    names = {"WC": WC, "WE": WE, "VA": VA, "VB": VB, "LA": LA, "LB": LB}

    def slot_of(name):
        for step in SCHEDULE.get(name, ()):
            m = names[step[1:3]]
            if m in (WC, WE):
                mixer_send(step[0], m)
            elif step[0] == "P":
                phase1(m)
            else:
                send(step[0], m, step[3])

    def gather(buf, k, gain, st, tag, early, late):
        z, xx, core = st
        cutoff = splits[k]
        z.wait_recv()
        zb = buf.at[c, blk(2)]
        zbt = buf.at[c, blk(2), pl.ds(0, cutoff)]
        diag = [go(rcopy(zbt, zbt, ags.at[k, 3], agr.at[k, 3], dev(dx=1)))]
        zcore = go(rcopy(zb, zb, ags.at[k, 4], agr.at[k, 4], dev(dc=1)))
        slot_of(tag + "0")
        xx.wait_recv()
        xb = buf.at[c, blk(1)]
        if cutoff < rows:
            xbb = buf.at[c, blk(1), pl.ds(cutoff, rows - cutoff)]
            diag.append(go(rcopy(xbb, xbb, ags.at[k, 5], agr.at[k, 5], dev(dzl=1))))
        xcore = go(rcopy(xb, xb, ags.at[k, 6], agr.at[k, 6], dev(dc=1)))
        slot_of(tag + "1")
        core.wait_recv()
        norm_block(buf, gain, blk(0))
        slot_of(tag + "2")
        zcore.wait_recv()
        norm_block(buf, gain, blk(2))
        slot_of(tag + "3")
        xcore.wait_recv()
        norm_block(buf, gain, blk(1))
        slot_of(tag + "4")
        early()
        for copy in diag:
            copy.wait_recv()
        db = buf.at[c, blk(3)]
        dcore = go(rcopy(db, db, ags.at[k, 7], agr.at[k, 7], dev(dc=1)))
        slot_of(tag + "5")
        dcore.wait_recv()
        norm_block(buf, gain, blk(3))
        slot_of(tag + "6")
        late()

    slot_of("a0")
    own = xa.at[c, y]
    xnear = go(rcopy(own, own, xs.at[0], xr.at[0], dev(dy=1)))
    xcore = go(rcopy(own, own, xs.at[1], xr.at[1], dev(dc=1)))
    slot_of("a1")
    loads["em"].wait()
    loads["es"].wait()
    for q in range(2):
        s_we[q] = (f_em[q * chan:(q + 1) * chan] * es[...]).astype(BF)
    slot_of("a2")
    loads["vv"].wait()
    loads["rv"].wait()
    for q in range(4):
        base = q * ff
        s_va[q, :, :cut] = f_vv[:, base:base + cut].astype(BF)
        s_va[q, :, cut:] = f_rv[:, base:base + cut].astype(BF)
    slot_of("a3")
    for q in range(4):
        base = q * ff
        s_vb[q, :, :ff - cut] = f_vv[:, base + cut:base + ff].astype(BF)
        s_vb[q, :, ff - cut:] = f_rv[:, base + cut:base + ff].astype(BF)
    slot_of("a4")
    loads["ls"].wait()
    loads["lw"].wait()
    for q in range(4):
        base = q * ff
        s_la[q] = (f_lw[base:base + cut] * ls[...]).astype(BF)
        s_lb[q] = (f_lw[base + cut:base + ff] * ls[...]).astype(BF)
    slot_of("a5")
    for name in ("g1", "sc", "sb", "gb", "offs", "loc", "g2", "sv", "sr"):
        loads[name].wait()
    head = lax.broadcasted_iota(jnp.int32, (offs_all.shape[0], chan), 0)
    lane = lax.broadcasted_iota(jnp.int32, (offs_all.shape[0], chan), 1)
    chosen = (lane >= (head - y * groups) * group_width) & (lane < (head - y * groups + 1) * group_width)
    offs[...] = lax.dot_general(
        offs_all[...], chosen.astype(F32), (((0,), (0,)), ((), ())),
        precision=lax.Precision.HIGHEST, preferred_element_type=F32,
    )
    slot = y * 2 + c
    xcore.wait_recv()
    norm_block(xa, g1, y)
    slot_of("b0")
    xnear.wait_recv()
    near = xa.at[c, 1 - y]
    xlast = go(rcopy(near, near, xs.at[2], xr.at[2], dev(dc=1)))
    slot_of("b1")
    xlast.wait_recv()
    norm_block(xa, g1, 1 - y)
    for name in ("b2", "b3", "b4", "b5"):
        slot_of(name)
    mixer_ready(WC)
    slot_of("c0")
    sc, sb, gb = (pick(v, chan, 0, chan) for v in (sc_all, sb_all, gb_all))
    for i, b in enumerate((y, 1 - y)):
        both = project(wc, b)
        car[b] = jax.nn.gelu(both[:, :chan] * sc)
        signal = jax.nn.gelu(both[:, chan:] * sb)
        sgn[b] = (signal * gb).astype(BF)
        sq[slot, b] = lax.dot_general(
            jnp.ones((8, chan), F32), signal * signal, (((1,), (1,)), ((), ())),
            precision=lax.Precision.HIGHEST, preferred_element_type=F32,
        )
        slot_of(f"c{i + 1}")
    squares = [
        go(rcopy(sq.at[slot], sq.at[slot], sqs.at[i], sqr.at[i], dev(dy=dy, dc=dc)))
        for i, (dy, dc) in enumerate(((1, 0), (1, 1), (0, 1)))
    ]
    slot_of("d0")
    for copy in squares:
        copy.wait_recv()
    slot_of("d1")
    lower = lax.broadcasted_iota(jnp.int32, (block_len, block_len), 0) >= lax.broadcasted_iota(
        jnp.int32, (block_len, block_len), 1
    )
    pack = max(1, 128 // group_width)
    wide = pack * group_width
    lane = lax.broadcasted_iota(jnp.int32, (block_len, wide), 1)
    mixer_ready(WE)
    slot_of("d2")
    cores1 = {}
    for i, b in enumerate((1 - y, y)):
        total = sq[0, b]
        for j in range(1, 4):
            total = total + sq[j, b]
        factor = lax.rsqrt(total / total_chan + EPS)
        for s in range(rows // block_len):
            span = slice(s * block_len, (s + 1) * block_len)
            for j in range(groups // pack):
                lanes = slice(j * wide, (j + 1) * wide)
                values = sgn[b, span, lanes]
                mixed = jnp.zeros((block_len, wide), F32)
                for g in range(pack):
                    mat = jnp.where(lower, loc[j * pack + g].astype(F32), 0.0) * factor[0:1, span]
                    one = jnp.dot(mat.astype(BF), values, preferred_element_type=F32)
                    inside = (lane >= g * group_width) & (lane < (g + 1) * group_width)
                    mixed = jnp.where(inside, one, mixed)
                gat[b, span, lanes] = (car[b, span, lanes] * (mixed + offs[:, lanes])).astype(BF)
        emit(b)
        cores1[i] = rcopy(part.at[1 - c, b], mcore.at[b], ms.at[i], mr.at[i], dev(dc=1))
        cores1[i].start()
        if i == 0:
            slot_of("d3")
    cores1[0].wait_recv()
    mhalf[...] = (part[c, 1 - y].astype(F32) + mcore[1 - y].astype(F32)).astype(BF)
    across = go(rcopy(mhalf, ry, ms.at[2], mr.at[2], dev(dy=1)))
    slot_of("e0")
    cores1[1].wait_recv()
    slot_of("e1")
    across.wait_recv()
    for i in range(2):
        cores1[i].wait_send()
    summed = part[c, y].astype(F32) + mcore[y].astype(F32) + ry[...].astype(F32)
    xm[c, ai] = (xa[c, y].astype(F32) + summed).astype(BF)
    st2 = gather_start(xm, 0)
    slot_of("e2")

    def up_projection(w, lo, hi, da):
        b = blk(da)
        sv, sr = (pick(v, ff, lo, hi) for v in (sv_all, sr_all))
        both = project(w, b)
        gate = both[:, :hi - lo] * sv
        up = both[:, hi - lo:] * sr
        hid[b, :, lo:hi] = (jax.nn.silu(gate) * up).astype(BF)

    ups = ((VA, va, 0, cut, "g"), (VB, vb, cut, ff, "h"))

    def second_early():
        for m, w, lo, hi, tag in ups:
            ready(m)
            slot_of(tag + "0")
            for i, da in enumerate((0, 2, 1)):
                up_projection(w, lo, hi, da)
                slot_of(f"{tag}{i + 1}")

    def second_late():
        for m, w, lo, hi, tag in ups:
            up_projection(w, lo, hi, 3)
            slot_of(tag + "4")

    gather(xm, 0, g2, st2, "f", second_early, second_late)
    cores2 = scatter_cores(0)
    plan2 = scatter_links(0)
    for far in range(2):
        a = 1 - zh if far else zh
        for off in range(2):
            p = 1 - y if off else y
            if off:
                for m in (LA, LB):
                    ready(m, "YF"[far])
            for i, da in enumerate(order):
                emit_plane(blk(da), a, p)
                if off:

                    @pl.when(c != a)
                    def _():
                        cores2[da].start()

            if not far:
                slot_of(f"i{off}")

        @pl.when(c == a)
        def _():
            scatter_first(0, cores2, plan2)

    summed = scatter_second(0, cores2, plan2, "j")
    out[...] = (xm[c, ai].astype(F32) + summed).astype(BF)
    for copy in pending:
        copy.wait_send()


def on_device_fused(
    sequence_entries, former_norm_factor, conveyor_matrix, conveyor_rescalers,
    blend_value_matrix, blend_rescalers, blend_norm_factor, location_matrices,
    location_offsets, branch_emission_matrix, emission_rescalers, latter_norm_factor,
    valve_matrix, valve_rescalers, raising_matrix, raising_rescalers,
    lowering_matrix, lowering_rescalers,
):
    parts = 4
    rows, width = sequence_entries.shape
    depth, chans = conveyor_matrix.shape
    chan = chans // 2
    hidden = valve_matrix.shape[1]
    ff = hidden // parts
    cut = (ff // 2 + 127) // 128 * 128
    heads = location_matrices.shape[0]
    groups = heads // 2
    block_len = location_matrices.shape[1]
    group_width = chan // groups
    total_chan = chans * lax.axis_size("tp")
    cols = branch_emission_matrix.shape[1]
    args = (
        sequence_entries, former_norm_factor, conveyor_matrix, conveyor_rescalers,
        blend_value_matrix, blend_rescalers, blend_norm_factor, location_matrices,
        location_offsets, branch_emission_matrix, emission_rescalers, latter_norm_factor,
        valve_matrix, valve_rescalers, raising_matrix, raising_rescalers,
        lowering_matrix, lowering_rescalers,
    )
    vm = pltpu.VMEM
    dma = pltpu.SemaphoreType.DMA
    cube = (2, 2, 2, 2, depth)
    scratch = [
        vm((depth, chans), F32), vm((depth, chans), F32), vm((chans, cols), F32),
        vm((depth, hidden), F32), vm((depth, hidden), F32), vm((hidden, cols), F32),
        vm((groups, block_len, block_len), BF),
        vm((1, 2 * width), F32), vm((1, 2 * width), F32), vm((1, chans), F32), vm((1, chans), F32),
        vm((1, chans), F32), vm((1, hidden), F32), vm((1, hidden), F32), vm((1, cols), F32),
        vm((1, cols), F32), vm((heads, block_len), F32),
        vm((2, depth, 2 * chan), BF), vm((2, chan, cols), BF),
        vm((parts, depth, 2 * cut), BF), vm((parts, depth, 2 * (ff - cut)), BF),
        vm((parts, cut, cols), BF), vm((parts, ff - cut, cols), BF),
        vm(cube + (2 * chan,), BF), vm((2, 2, 2, chan, 2 * cols), BF),
        vm(cube + (2 * cut,), BF), vm(cube + (2 * (ff - cut),), BF),
        vm((2, 2, cut, 4 * cols), BF), vm((2, 2, ff - cut, 4 * cols), BF),
        vm((2, 2, rows, width), BF), vm((2, 4, rows, width), BF), vm((2, 4, rows, width), BF),
        vm((2, rows, chan), F32), vm((2, rows, chan), BF), vm((2, rows, chan), BF),
        vm((4, rows, ff), BF), vm((4, 2, 8, rows), F32), vm((block_len, chan), F32),
        vm((2, 4, rows, width), BF), vm((1, 4, rows, width), BF), vm((1, 4, rows, width), BF),
        vm((1, rows, width), BF), vm((1, rows, width), BF),
        vm((1, rows, width), BF), vm((1, rows, width), BF),
        vm((rows, width), BF), vm((2, rows, width), BF), vm((rows, width), BF),
        dma((18,)), dma((6, 3)), dma((6, 3)), dma((6,)), dma((6, 6)), dma((6, 6)),
        dma((1, 8)), dma((1, 8)), dma((3,)), dma((3,)), dma((1, 10)), dma((1, 10)),
        dma((2, 8)), dma((2, 8)), dma((3,)), dma((3,)), dma((3,)), dma((3,)),
    ]
    splits = tuple(rows * part // 16 for part in SPLITS)
    dims = (rows, width, chan, ff, cut, block_len, group_width, total_chan, splits)
    return pl.pallas_call(
        functools.partial(layer_kernel, dims),
        out_shape=jax.ShapeDtypeStruct((rows, width), BF),
        in_specs=[pl.BlockSpec(memory_space=pl.ANY)] * len(args),
        out_specs=pl.BlockSpec(memory_space=pltpu.VMEM),
        scratch_shapes=scratch,
        compiler_params=pltpu.CompilerParams(
            collective_id=0, has_side_effects=True, vmem_limit_bytes=66000000
        ),
    )(*args)


def normalize(rows, gain):
    values = rows.astype(jnp.float32)
    factor = lax.rsqrt(jnp.mean(values * values, axis=-1, keepdims=True) + EPS)
    return (values * factor * gain).astype(jnp.bfloat16)


def elementwise_plus(left_rows, pieces):
    return (
        jnp.dot(left_rows, pieces[0], preferred_element_type=jnp.float32),
        jnp.dot(left_rows, pieces[1], preferred_element_type=jnp.float32),
    )


def project_cols(left_rows, scales, piece):
    return jnp.dot(left_rows, piece, preferred_element_type=jnp.float32) * scales


def on_device(
    sequence_entries,
    former_norm_factor,
    conveyor_matrix,
    conveyor_rescalers,
    blend_value_matrix,
    blend_rescalers,
    blend_norm_factor,
    location_matrices,
    location_offsets,
    branch_emission_matrix,
    emission_rescalers,
    latter_norm_factor,
    valve_matrix,
    valve_rescalers,
    raising_matrix,
    raising_rescalers,
    lowering_matrix,
    lowering_rescalers,
):
    out_scales, down_scales = (
        lax.all_gather(emission_rescalers, "fs", axis=0, tiled=True),
        lax.all_gather(lowering_rescalers, "fs", axis=0, tiled=True),
    )
    full_rows = lax.all_gather(sequence_entries, "tp", axis=1, tiled=True)
    own_width = sequence_entries.shape[1]
    own_start = lax.axis_index("tp") * own_width
    standardized_source = normalize(full_rows, former_norm_factor)
    conveyor_prior, stream_prior = elementwise_plus(
        standardized_source,
        (
            lax.all_gather(conveyor_matrix.astype(jnp.bfloat16), "fs", axis=0, tiled=True),
            lax.all_gather(blend_value_matrix.astype(jnp.bfloat16), "fs", axis=0, tiled=True),
        ),
    )
    conveyor_current = jax.nn.gelu(conveyor_prior * conveyor_rescalers)
    signal = jax.nn.gelu(stream_prior * blend_rescalers)
    total_sq = lax.psum(jnp.sum(signal * signal, axis=1), "tp")
    channels = signal.shape[1] * lax.axis_size("tp")
    signal_norm = (
        signal * lax.rsqrt(total_sq / channels + EPS)[:, None] * blend_norm_factor
    ).astype(jnp.bfloat16)
    local_groups = location_matrices.shape[0]
    block_len = location_matrices.shape[1]
    group_width = signal.shape[1] // local_groups
    lower_mask = jnp.tril(jnp.ones((block_len, block_len), bool))
    masked = jnp.where(lower_mask[None], location_matrices, jnp.zeros((), jnp.bfloat16))
    signal_blocks = signal_norm.reshape(-1, block_len, local_groups, group_width)
    location_blended = jnp.einsum(
        "gts,bsgd->btgd", masked, signal_blocks, preferred_element_type=jnp.float32
    )
    location_blended = location_blended + location_offsets.T[None, :, :, None]
    filtered_result = (conveyor_current * location_blended.reshape(conveyor_current.shape)).astype(
        jnp.bfloat16
    )
    mixer_terms = project_cols(
        filtered_result,
        out_scales,
        lax.all_gather(branch_emission_matrix.astype(jnp.bfloat16), "fs", axis=1, tiled=True),
    )
    summed = lax.psum(mixer_terms.astype(jnp.bfloat16), "tp").astype(jnp.float32)
    mid_rows = (full_rows.astype(jnp.float32) + summed).astype(jnp.bfloat16)
    mid_own = lax.dynamic_slice_in_dim(mid_rows, own_start, own_width, 1)
    ffn_in = normalize(mid_rows, latter_norm_factor)
    gate_half = valve_matrix.astype(jnp.bfloat16)
    up_half = raising_matrix.astype(jnp.bfloat16)
    whole_gate, whole_up = (
        lax.all_gather(gate_half, "fs", axis=0, tiled=True),
        lax.all_gather(up_half, "fs", axis=0, tiled=True),
    )
    pre_gate = jnp.dot(ffn_in, whole_gate, preferred_element_type=jnp.float32)
    pre_up = jnp.dot(ffn_in, whole_up, preferred_element_type=jnp.float32)
    hidden = (jax.nn.silu(pre_gate * valve_rescalers) * (pre_up * raising_rescalers)).astype(
        jnp.bfloat16
    )
    ffn_terms = project_cols(
        hidden,
        down_scales,
        lax.all_gather(lowering_matrix.astype(jnp.bfloat16), "fs", axis=1, tiled=True),
    )
    ffn_share = lax.psum_scatter(
        ffn_terms.astype(jnp.bfloat16), "tp", scatter_dimension=1, tiled=True
    ).astype(jnp.float32)
    return (mid_own.astype(jnp.float32) + ffn_share).astype(jnp.bfloat16)


def solution(mesh):
    sizes = dict(mesh.shape)
    fused = sizes["tp"] == 2 and sizes["fs"] == 16
    return jax.shard_map(
        on_device_fused if fused else on_device,
        mesh=mesh,
        in_specs=(
            P("fs", "tp"),
            P(),
            P("fs", "tp"),
            P("tp"),
            P("fs", "tp"),
            P("tp"),
            P("tp"),
            P("tp", None, None),
            P("tp", None),
            P("tp", "fs"),
            P("fs"),
            P(),
            P("fs", "tp"),
            P("tp"),
            P("fs", "tp"),
            P("tp"),
            P("tp", "fs"),
            P("fs"),
        ),
        out_specs=P("fs", "tp"),
        check_vma=False,
    )
```

```python
import functools

import jax
import jax.numpy as jnp
from jax import lax
from jax.experimental import pallas as pl
from jax.experimental.pallas import tpu as pltpu
from jax.sharding import PartitionSpec as P

EPS = 1e-06
MESH = pl.DeviceIdType.MESH
BF = jnp.bfloat16
F32 = jnp.float32
SCHEDULE = {
    "a0": ("PWC",),
    "a3": ("PVA", "XWC",),
    "a4": ("HWC", "PWE", "LWC",),
    "a5": ("MWC",),
    "b0": ("VWC", "ZVAb",),
    "b1": ("PVB", "YVAb", "UWC",),
    "b2": ("YVAa", "QWC",),
    "b3": ("HWE", "FVAb",),
    "b4": ("ZVAa", "YVBa", "XWE",),
    "b5": ("MWE", "YVBb",),
    "c0": ("LWE",),
    "c1": ("ZVBb", "PLB",),
    "c2": ("VWE",),
    "d0": ("ZVBa", "QWE", "FVAa", "UWE",),
    "d2": ("YLBa",),
    "d3": ("PLA",),
    "e0": ("YLAb", "YLAa", "FVBa", "FVBb",),
    "e1": ("ZLBb",),
    "e2": ("ZLAb",),
    "f1": ("YLBb", "FLBb",),
    "f2": ("ZLBa", "ZLAa",),
    "g1": ("FLAb",),
    "f6": ("FLBa",),
    "i1": ("FLAa",),
}
SPLITS = (9, 8)


def layer_kernel(
    dims,
    x_in, g1_in, cv_in, sc_in, bv_in, sb_in, gb_in, loc_in, offs_in, em_in, es_in,
    g2_in, vv_in, sv_in, rv_in, sr_in, lw_in, ls_in,
    out,
    f_cv, f_bv, f_em, f_vv, f_rv, f_lw, loc,
    g1, g2, sc_all, sb_all, gb_all, sv_all, sr_all, es, ls, offs_all,
    s_wc, s_we, s_va, s_vb, s_la, s_lb,
    wc, we, va, vb, la, lb,
    xa, xm, nrm, car, sgn, gat, hid, sq, offs, part, half, rcore, rx, rz, dx_in, dz_in, mhalf, mcore, ry,
    inl, p1s, p1r, p1l, p2s, p2r, ags, agr, sqs, sqr, rss, rsr, ws, wr, xs, xr, ms, mr,
):
    rows, width, chan, ff, cut, block_len, group_width, total_chan, splits = dims
    fs = lax.axis_index("fs")
    c = lax.axis_index("tp")
    x = fs % 2
    y = (fs // 2) % 2
    zl = (fs // 4) % 2
    zh = fs // 8
    ai = x + 2 * zl
    groups = chan // group_width

    def dev(dx=0, dy=0, dzl=0, dzh=0, dc=0):
        nx = 1 - x if dx else x
        ny = 1 - y if dy else y
        nzl = 1 - zl if dzl else zl
        nzh = 1 - zh if dzh else zh
        nc = 1 - c if dc else c
        return {"fs": nzh * 8 + nzl * 4 + ny * 2 + nx, "tp": nc}

    def blk(da):
        return (1 - x if da & 1 else x) + 2 * (1 - zl if da & 2 else zl)

    loads = {}

    def load(name, src, dst):
        copy = pltpu.make_async_copy(src, dst, inl.at[len(loads)])
        copy.start()
        loads[name] = copy

    load("cv", cv_in, f_cv)
    load("bv", bv_in, f_bv)
    load("x", x_in, xa.at[c, y])
    load("em", em_in, f_em)
    load("es", es_in, es.at[0])
    load("vv", vv_in, f_vv)
    load("rv", rv_in, f_rv)
    load("ls", ls_in, ls.at[0])
    load("lw", lw_in, f_lw)
    for name, src, dst in (
        ("g1", g1_in, g1.at[0]), ("sc", sc_in, sc_all.at[0]), ("sb", sb_in, sb_all.at[0]), ("gb", gb_in, gb_all.at[0]),
        ("offs", offs_in, offs_all), ("loc", loc_in.at[pl.ds(y * groups, groups)], loc),
        ("g2", g2_in, g2.at[0]), ("sv", sv_in, sv_all.at[0]), ("sr", sr_in, sr_all.at[0]),
    ):
        load(name, src, dst)

    peers = [dev(dx=da & 1, dzl=da & 2, dc=dc) for da in range(4) for dc in range(2) if da or dc]
    peers += [dev(dy=1), dev(dy=1, dc=1), dev(dzh=1)]
    barrier = pltpu.get_barrier_semaphore()
    for peer in peers:
        pl.semaphore_signal(barrier, inc=1, device_id=peer, device_id_type=MESH)

    loads["cv"].wait()
    loads["bv"].wait()
    for q in range(2):
        s_wc[q, :, :chan] = f_cv[:, q * chan:(q + 1) * chan].astype(BF)
        s_wc[q, :, chan:] = f_bv[:, q * chan:(q + 1) * chan].astype(BF)
    loads["x"].wait()
    pl.semaphore_wait(barrier, len(peers))

    def rcopy(src, dst, ss, rs, to):
        return pltpu.make_async_remote_copy(
            src_ref=src, dst_ref=dst, send_sem=ss, recv_sem=rs, device_id=to, device_id_type=MESH
        )

    pending = []

    def go(copy):
        copy.start()
        pending.append(copy)
        return copy

    ins = (s_wc, s_we, s_va, s_vb, s_la, s_lb)
    dst = (wc, we, va, vb, la, lb)
    rowwise = (False, True, False, False, True, True)
    WC, WE, VA, VB, LA, LB = range(6)

    def cell(m):
        if m == WE:
            lanes = ins[m].shape[2]
            return we.at[zh, zl, x, :, pl.ds(pl.multiple_of(y * lanes, lanes), lanes)]
        if rowwise[m]:
            lanes = ins[m].shape[2]
            return dst[m].at[zh, zl, :, pl.ds(pl.multiple_of((y * 2 + x) * lanes, lanes), lanes)]
        return dst[m].at[zh, zl, y, x]

    def level(m, a, b):
        return we.at[a, b, x] if m == WE else wc.at[a, b, :, x]

    first = {}
    moved = {}
    landed = set()

    def mixer_send(kind, m):
        i = "PLHXMUVQ".index(kind)

        def move(src, to, into=None):
            moved[kind, m] = go(rcopy(src, src if into is None else into, ws.at[m, i], wr.at[m, i], to))

        if kind == "P":
            first[m] = pltpu.make_async_copy(ins[m].at[y], cell(m), p1l.at[m])
            first[m].start()
            move(ins[m].at[1 - y], dev(dy=1), cell(m))
            return
        if m in first:
            first.pop(m).wait()
            moved["P", m].wait_recv()
        source = {"U": "L", "V": "H", "M": "H", "Q": "M"}.get(kind)
        if source and (source, m) not in landed:
            landed.add((source, m))
            moved[source, m].wait_recv()
        far, other = kind in "MVQ", kind in "UQ"
        src = level(m, 1 - zh if far else zh, 1 - zl if other else zl)
        move(src, dev(dzh=1) if kind == "H" else dev(dzl=1) if kind in "LM" else dev(dx=1))

    def mixer_ready(m):
        for kind in "XUVQ":
            moved[kind, m].wait_recv()

    def piece(m, a, b, h):
        level = 1 - zl if h == "b" else zl
        if rowwise[m]:
            lanes = 2 * ins[m].shape[2]
            return dst[m].at[a, level, :, pl.ds(pl.multiple_of(b * lanes, lanes), lanes)]
        return dst[m].at[a, level, b]

    second = {}

    def phase1(m):
        local = pltpu.make_async_copy(ins[m].at[ai], cell(m), p1l.at[m])
        local.start()
        copies = {
            da: go(rcopy(ins[m].at[blk(da)], cell(m), p1s.at[m, da - 1], p1r.at[m, da - 1], dev(dx=da & 1, dzl=da & 2)))
            for da in (3, 2, 1)
        }
        first[m, "a"] = (local, copies[1])
        first[m, "b"] = (copies[2], copies[3])

    def settle(m, h):
        if (m, h) in first:
            one, two = first.pop((m, h))
            two.wait_recv()
            if h == "a":
                one.wait()
            else:
                one.wait_recv()

    def send(kind, m, h):
        i = "ZYF".index(kind) * 2 + "ab".index(h)
        if kind == "F":
            second["Z", m, h].wait_recv()
            src = piece(m, 1 - zh, y, h)
        else:
            settle(m, h)
            src = piece(m, zh, y, h)
        to = dev(dzh=1) if kind == "Z" else dev(dy=1)
        second[kind, m, h] = go(rcopy(src, src, p2s.at[m, i], p2r.at[m, i], to))

    def ready(m, kinds="YF"):
        for kind in kinds:
            for h in "ab":
                second[kind, m, h].wait_recv()

    def gather_start(buf, k):
        own = buf.at[c, ai]
        z = go(rcopy(own, own, ags.at[k, 0], agr.at[k, 0], dev(dzl=1)))
        xx = go(rcopy(own, own, ags.at[k, 1], agr.at[k, 1], dev(dx=1)))
        core = go(rcopy(own, own, ags.at[k, 2], agr.at[k, 2], dev(dc=1)))
        return [z, xx, core]

    def norm_block(buf, gain, b):
        total = jnp.zeros((rows, 1), F32)
        for h in range(2):
            v = buf[h, b].astype(F32)
            total = total + jnp.sum(v * v, axis=-1, keepdims=True)
        factor = lax.rsqrt(total / (2 * width) + EPS)
        for h in range(2):
            nrm[h, b] = (buf[h, b].astype(F32) * factor * gain[:, h * width:(h + 1) * width]).astype(BF)

    def project(w, b):
        n = w.shape[-1]
        return jnp.dot(nrm[0, b], w[0].reshape(width, n), preferred_element_type=F32) + jnp.dot(
            nrm[1, b], w[1].reshape(width, n), preferred_element_type=F32
        )

    def emit(b):
        v = gat[b]
        n = s_we.shape[-1]
        for h in range(2):
            for q in range(2):
                for xx in range(2):
                    both = jnp.dot(v, we[h, q, xx], preferred_element_type=F32).astype(BF)
                    for yy in range(2):
                        at = ((q * 2 + yy) * 2 + xx) * n
                        part[h, b, :, at:at + n] = both[:, yy * n:(yy + 1) * n]

    def emit_plane(b, a, p):
        n = 2 * s_la.shape[2]
        lanes = pl.ds(pl.multiple_of(p * n, n), n)
        for q in range(2):
            at = pl.ds(pl.multiple_of(q * 2 * n + p * n, n), n)
            part[a, b, :, at] = (
                jnp.dot(hid[b, :, :cut], la[a, q, :, lanes], preferred_element_type=F32)
                + jnp.dot(hid[b, :, cut:], lb[a, q, :, lanes], preferred_element_type=F32)
            ).astype(BF)

    order = (3, 1, 2, 0)

    def scatter_cores(k):
        cores = {
            da: rcopy(part.at[1 - c, blk(da)], rcore.at[k, blk(da)], rss.at[k, i], rsr.at[k, i], dev(dc=1))
            for i, da in enumerate(order)
        }
        return cores

    def scatter_links(k):
        cutoff = splits[1 + k]
        rest = rows - cutoff
        top, bottom = pl.ds(0, cutoff), pl.ds(cutoff, rest)
        zb, xb, db = blk(2), blk(1), blk(3)
        links = {
            "dx": rcopy(half.at[k, db, top], dx_in.at[k, top], rss.at[k, 4], rsr.at[k, 4], dev(dx=1)),
            "x0": rcopy(half.at[k, xb, top], rx.at[k, top], rss.at[k, 7], rsr.at[k, 7], dev(dx=1)),
            "z1": rcopy(half.at[k, zb, top], rz.at[k, top], rss.at[k, 8], rsr.at[k, 8], dev(dzl=1)),
        }
        if rest:
            links["dz"] = rcopy(
                half.at[k, db, bottom], dz_in.at[k, bottom], rss.at[k, 5], rsr.at[k, 5], dev(dzl=1)
            )
            links["z0"] = rcopy(half.at[k, zb, bottom], rz.at[k, bottom], rss.at[k, 6], rsr.at[k, 6], dev(dzl=1))
            links["x1"] = rcopy(half.at[k, xb, bottom], rx.at[k, bottom], rss.at[k, 9], rsr.at[k, 9], dev(dx=1))
        pending.extend(links.values())
        return links, top, bottom

    def scatter_first(k, cores, plan):
        links, top, bottom = plan

        def combine(da):
            b = blk(da)
            cores[da].wait_recv()
            half[k, b] = (part[c, b].astype(F32) + rcore[k, b].astype(F32)).astype(BF)

        combine(3)
        links["dx"].start()
        if "dz" in links:
            links["dz"].start()
        combine(1)
        links["x0"].start()
        combine(2)
        if "z0" in links:
            links["z0"].start()

    def scatter_second(k, cores, plan, tag):
        links, top, bottom = plan
        zb, xb = blk(2), blk(1)
        slot_of(tag + "0")
        links["dx"].wait_recv()
        half[k, zb, top] = (half[k, zb, top].astype(F32) + dx_in[k, top].astype(F32)).astype(BF)
        links["z1"].start()
        if "dz" in links:
            links["dz"].wait_recv()
            half[k, xb, bottom] = (half[k, xb, bottom].astype(F32) + dz_in[k, bottom].astype(F32)).astype(BF)
            links["x1"].start()
        slot_of(tag + "1")
        cores[0].wait_recv()
        for da in order:
            cores[da].wait_send()
        own = part[c, ai].astype(F32) + rcore[k, ai].astype(F32)
        for name in ("x0", "z0", "z1", "x1"):
            if name in links:
                links[name].wait_recv()
        return own + rz[k].astype(F32) + rx[k].astype(F32)

    def pick(ref, n, lo, hi):
        value = ref[:, lo:hi]
        for k in range(1, ref.shape[1] // n):
            value = jnp.where((ai if ref.shape[1] // n == 4 else y) == k, ref[:, k * n + lo:k * n + hi], value)
        return value

    names = {"WC": WC, "WE": WE, "VA": VA, "VB": VB, "LA": LA, "LB": LB}

    def slot_of(name):
        for step in SCHEDULE.get(name, ()):
            m = names[step[1:3]]
            if m in (WC, WE):
                mixer_send(step[0], m)
            elif step[0] == "P":
                phase1(m)
            else:
                send(step[0], m, step[3])

    def gather(buf, k, gain, st, tag, early, late):
        z, xx, core = st
        cutoff = splits[k]
        z.wait_recv()
        zb = buf.at[c, blk(2)]
        zbt = buf.at[c, blk(2), pl.ds(0, cutoff)]
        diag = [go(rcopy(zbt, zbt, ags.at[k, 3], agr.at[k, 3], dev(dx=1)))]
        zcore = go(rcopy(zb, zb, ags.at[k, 4], agr.at[k, 4], dev(dc=1)))
        slot_of(tag + "0")
        xx.wait_recv()
        xb = buf.at[c, blk(1)]
        if cutoff < rows:
            xbb = buf.at[c, blk(1), pl.ds(cutoff, rows - cutoff)]
            diag.append(go(rcopy(xbb, xbb, ags.at[k, 5], agr.at[k, 5], dev(dzl=1))))
        xcore = go(rcopy(xb, xb, ags.at[k, 6], agr.at[k, 6], dev(dc=1)))
        slot_of(tag + "1")
        core.wait_recv()
        norm_block(buf, gain, blk(0))
        slot_of(tag + "2")
        zcore.wait_recv()
        norm_block(buf, gain, blk(2))
        slot_of(tag + "3")
        xcore.wait_recv()
        norm_block(buf, gain, blk(1))
        slot_of(tag + "4")
        early()
        for copy in diag:
            copy.wait_recv()
        db = buf.at[c, blk(3)]
        dcore = go(rcopy(db, db, ags.at[k, 7], agr.at[k, 7], dev(dc=1)))
        slot_of(tag + "5")
        dcore.wait_recv()
        norm_block(buf, gain, blk(3))
        slot_of(tag + "6")
        late()

    slot_of("a0")
    own = xa.at[c, y]
    xnear = go(rcopy(own, own, xs.at[0], xr.at[0], dev(dy=1)))
    xcore = go(rcopy(own, own, xs.at[1], xr.at[1], dev(dc=1)))
    slot_of("a1")
    loads["em"].wait()
    loads["es"].wait()
    for q in range(2):
        s_we[q] = (f_em[q * chan:(q + 1) * chan] * es[...]).astype(BF)
    slot_of("a2")
    loads["vv"].wait()
    loads["rv"].wait()
    for q in range(4):
        base = q * ff
        s_va[q, :, :cut] = f_vv[:, base:base + cut].astype(BF)
        s_va[q, :, cut:] = f_rv[:, base:base + cut].astype(BF)
    slot_of("a3")
    for q in range(4):
        base = q * ff
        s_vb[q, :, :ff - cut] = f_vv[:, base + cut:base + ff].astype(BF)
        s_vb[q, :, ff - cut:] = f_rv[:, base + cut:base + ff].astype(BF)
    slot_of("a4")
    loads["ls"].wait()
    loads["lw"].wait()
    for q in range(4):
        base = q * ff
        s_la[q] = (f_lw[base:base + cut] * ls[...]).astype(BF)
        s_lb[q] = (f_lw[base + cut:base + ff] * ls[...]).astype(BF)
    slot_of("a5")
    for name in ("g1", "sc", "sb", "gb", "offs", "loc", "g2", "sv", "sr"):
        loads[name].wait()
    head = lax.broadcasted_iota(jnp.int32, (offs_all.shape[0], chan), 0)
    lane = lax.broadcasted_iota(jnp.int32, (offs_all.shape[0], chan), 1)
    chosen = (lane >= (head - y * groups) * group_width) & (lane < (head - y * groups + 1) * group_width)
    offs[...] = lax.dot_general(
        offs_all[...], chosen.astype(F32), (((0,), (0,)), ((), ())),
        precision=lax.Precision.HIGHEST, preferred_element_type=F32,
    )
    slot = y * 2 + c
    xcore.wait_recv()
    norm_block(xa, g1, y)
    slot_of("b0")
    xnear.wait_recv()
    near = xa.at[c, 1 - y]
    xlast = go(rcopy(near, near, xs.at[2], xr.at[2], dev(dc=1)))
    slot_of("b1")
    xlast.wait_recv()
    norm_block(xa, g1, 1 - y)
    for name in ("b2", "b3", "b4", "b5"):
        slot_of(name)
    mixer_ready(WC)
    slot_of("c0")
    sc, sb, gb = (pick(v, chan, 0, chan) for v in (sc_all, sb_all, gb_all))
    for i, b in enumerate((y, 1 - y)):
        both = project(wc, b)
        car[b] = jax.nn.gelu(both[:, :chan] * sc)
        signal = jax.nn.gelu(both[:, chan:] * sb)
        sgn[b] = (signal * gb).astype(BF)
        sq[slot, b] = lax.dot_general(
            jnp.ones((8, chan), F32), signal * signal, (((1,), (1,)), ((), ())),
            precision=lax.Precision.HIGHEST, preferred_element_type=F32,
        )
        slot_of(f"c{i + 1}")
    squares = [
        go(rcopy(sq.at[slot], sq.at[slot], sqs.at[i], sqr.at[i], dev(dy=dy, dc=dc)))
        for i, (dy, dc) in enumerate(((1, 0), (1, 1), (0, 1)))
    ]
    slot_of("d0")
    for copy in squares:
        copy.wait_recv()
    slot_of("d1")
    lower = lax.broadcasted_iota(jnp.int32, (block_len, block_len), 0) >= lax.broadcasted_iota(
        jnp.int32, (block_len, block_len), 1
    )
    pack = max(1, 128 // group_width)
    wide = pack * group_width
    lane = lax.broadcasted_iota(jnp.int32, (block_len, wide), 1)
    mixer_ready(WE)
    slot_of("d2")
    cores1 = {}
    for i, b in enumerate((1 - y, y)):
        total = sq[0, b]
        for j in range(1, 4):
            total = total + sq[j, b]
        factor = lax.rsqrt(total / total_chan + EPS)
        for s in range(rows // block_len):
            span = slice(s * block_len, (s + 1) * block_len)
            for j in range(groups // pack):
                lanes = slice(j * wide, (j + 1) * wide)
                values = sgn[b, span, lanes]
                mixed = jnp.zeros((block_len, wide), F32)
                for g in range(pack):
                    mat = jnp.where(lower, loc[j * pack + g].astype(F32), 0.0) * factor[0:1, span]
                    one = jnp.dot(mat.astype(BF), values, preferred_element_type=F32)
                    inside = (lane >= g * group_width) & (lane < (g + 1) * group_width)
                    mixed = jnp.where(inside, one, mixed)
                gat[b, span, lanes] = (car[b, span, lanes] * (mixed + offs[:, lanes])).astype(BF)
        emit(b)
        cores1[i] = rcopy(part.at[1 - c, b], mcore.at[b], ms.at[i], mr.at[i], dev(dc=1))
        cores1[i].start()
        if i == 0:
            slot_of("d3")
    cores1[0].wait_recv()
    mhalf[...] = (part[c, 1 - y].astype(F32) + mcore[1 - y].astype(F32)).astype(BF)
    across = go(rcopy(mhalf, ry, ms.at[2], mr.at[2], dev(dy=1)))
    slot_of("e0")
    cores1[1].wait_recv()
    slot_of("e1")
    across.wait_recv()
    for i in range(2):
        cores1[i].wait_send()
    summed = part[c, y].astype(F32) + mcore[y].astype(F32) + ry[...].astype(F32)
    xm[c, ai] = (xa[c, y].astype(F32) + summed).astype(BF)
    st2 = gather_start(xm, 0)
    slot_of("e2")

    def up_projection(w, lo, hi, da):
        b = blk(da)
        sv, sr = (pick(v, ff, lo, hi) for v in (sv_all, sr_all))
        both = project(w, b)
        gate = both[:, :hi - lo] * sv
        up = both[:, hi - lo:] * sr
        hid[b, :, lo:hi] = (jax.nn.silu(gate) * up).astype(BF)

    ups = ((VA, va, 0, cut, "g"), (VB, vb, cut, ff, "h"))

    def second_early():
        for m, w, lo, hi, tag in ups:
            ready(m)
            slot_of(tag + "0")
            for i, da in enumerate((0, 2, 1)):
                up_projection(w, lo, hi, da)
                slot_of(f"{tag}{i + 1}")

    def second_late():
        for m, w, lo, hi, tag in ups:
            up_projection(w, lo, hi, 3)
            slot_of(tag + "4")

    gather(xm, 0, g2, st2, "f", second_early, second_late)
    cores2 = scatter_cores(0)
    plan2 = scatter_links(0)
    for far in range(2):
        a = 1 - zh if far else zh
        for off in range(2):
            p = 1 - y if off else y
            if off:
                for m in (LA, LB):
                    ready(m, "YF"[far])
            for i, da in enumerate(order):
                emit_plane(blk(da), a, p)
                if off:

                    @pl.when(c != a)
                    def _():
                        cores2[da].start()

            if not far:
                slot_of(f"i{off}")

        @pl.when(c == a)
        def _():
            scatter_first(0, cores2, plan2)

    summed = scatter_second(0, cores2, plan2, "j")
    out[...] = (xm[c, ai].astype(F32) + summed).astype(BF)
    for copy in pending:
        copy.wait_send()


def on_device_fused(
    sequence_entries, former_norm_factor, conveyor_matrix, conveyor_rescalers,
    blend_value_matrix, blend_rescalers, blend_norm_factor, location_matrices,
    location_offsets, branch_emission_matrix, emission_rescalers, latter_norm_factor,
    valve_matrix, valve_rescalers, raising_matrix, raising_rescalers,
    lowering_matrix, lowering_rescalers,
):
    parts = 4
    rows, width = sequence_entries.shape
    depth, chans = conveyor_matrix.shape
    chan = chans // 2
    hidden = valve_matrix.shape[1]
    ff = hidden // parts
    cut = (ff // 2 + 127) // 128 * 128
    heads = location_matrices.shape[0]
    groups = heads // 2
    block_len = location_matrices.shape[1]
    group_width = chan // groups
    total_chan = chans * lax.axis_size("tp")
    cols = branch_emission_matrix.shape[1]
    args = (
        sequence_entries, former_norm_factor, conveyor_matrix, conveyor_rescalers,
        blend_value_matrix, blend_rescalers, blend_norm_factor, location_matrices,
        location_offsets, branch_emission_matrix, emission_rescalers, latter_norm_factor,
        valve_matrix, valve_rescalers, raising_matrix, raising_rescalers,
        lowering_matrix, lowering_rescalers,
    )
    vm = pltpu.VMEM
    dma = pltpu.SemaphoreType.DMA
    cube = (2, 2, 2, 2, depth)
    scratch = [
        vm((depth, chans), F32), vm((depth, chans), F32), vm((chans, cols), F32),
        vm((depth, hidden), F32), vm((depth, hidden), F32), vm((hidden, cols), F32),
        vm((groups, block_len, block_len), BF),
        vm((1, 2 * width), F32), vm((1, 2 * width), F32), vm((1, chans), F32), vm((1, chans), F32),
        vm((1, chans), F32), vm((1, hidden), F32), vm((1, hidden), F32), vm((1, cols), F32),
        vm((1, cols), F32), vm((heads, block_len), F32),
        vm((2, depth, 2 * chan), BF), vm((2, chan, cols), BF),
        vm((parts, depth, 2 * cut), BF), vm((parts, depth, 2 * (ff - cut)), BF),
        vm((parts, cut, cols), BF), vm((parts, ff - cut, cols), BF),
        vm(cube + (2 * chan,), BF), vm((2, 2, 2, chan, 2 * cols), BF),
        vm(cube + (2 * cut,), BF), vm(cube + (2 * (ff - cut),), BF),
        vm((2, 2, cut, 4 * cols), BF), vm((2, 2, ff - cut, 4 * cols), BF),
        vm((2, 2, rows, width), BF), vm((2, 4, rows, width), BF), vm((2, 4, rows, width), BF),
        vm((2, rows, chan), F32), vm((2, rows, chan), BF), vm((2, rows, chan), BF),
        vm((4, rows, ff), BF), vm((4, 2, 8, rows), F32), vm((block_len, chan), F32),
        vm((2, 4, rows, width), BF), vm((1, 4, rows, width), BF), vm((1, 4, rows, width), BF),
        vm((1, rows, width), BF), vm((1, rows, width), BF),
        vm((1, rows, width), BF), vm((1, rows, width), BF),
        vm((rows, width), BF), vm((2, rows, width), BF), vm((rows, width), BF),
        dma((18,)), dma((6, 3)), dma((6, 3)), dma((6,)), dma((6, 6)), dma((6, 6)),
        dma((1, 8)), dma((1, 8)), dma((3,)), dma((3,)), dma((1, 10)), dma((1, 10)),
        dma((2, 8)), dma((2, 8)), dma((3,)), dma((3,)), dma((3,)), dma((3,)),
    ]
    splits = tuple(rows * part // 16 for part in SPLITS)
    dims = (rows, width, chan, ff, cut, block_len, group_width, total_chan, splits)
    return pl.pallas_call(
        functools.partial(layer_kernel, dims),
        out_shape=jax.ShapeDtypeStruct((rows, width), BF),
        in_specs=[pl.BlockSpec(memory_space=pl.ANY)] * len(args),
        out_specs=pl.BlockSpec(memory_space=pltpu.VMEM),
        scratch_shapes=scratch,
        compiler_params=pltpu.CompilerParams(
            collective_id=0, has_side_effects=True, vmem_limit_bytes=66000000
        ),
    )(*args)


def normalize(rows, gain):
    values = rows.astype(jnp.float32)
    factor = lax.rsqrt(jnp.mean(values * values, axis=-1, keepdims=True) + EPS)
    return (values * factor * gain).astype(jnp.bfloat16)


def elementwise_plus(left_rows, pieces):
    return (
        jnp.dot(left_rows, pieces[0], preferred_element_type=jnp.float32),
        jnp.dot(left_rows, pieces[1], preferred_element_type=jnp.float32),
    )


def project_cols(left_rows, scales, piece):
    return jnp.dot(left_rows, piece, preferred_element_type=jnp.float32) * scales


def on_device(
    sequence_entries,
    former_norm_factor,
    conveyor_matrix,
    conveyor_rescalers,
    blend_value_matrix,
    blend_rescalers,
    blend_norm_factor,
    location_matrices,
    location_offsets,
    branch_emission_matrix,
    emission_rescalers,
    latter_norm_factor,
    valve_matrix,
    valve_rescalers,
    raising_matrix,
    raising_rescalers,
    lowering_matrix,
    lowering_rescalers,
):
    out_scales, down_scales = (
        lax.all_gather(emission_rescalers, "fs", axis=0, tiled=True),
        lax.all_gather(lowering_rescalers, "fs", axis=0, tiled=True),
    )
    full_rows = lax.all_gather(sequence_entries, "tp", axis=1, tiled=True)
    own_width = sequence_entries.shape[1]
    own_start = lax.axis_index("tp") * own_width
    standardized_source = normalize(full_rows, former_norm_factor)
    conveyor_prior, stream_prior = elementwise_plus(
        standardized_source,
        (
            lax.all_gather(conveyor_matrix.astype(jnp.bfloat16), "fs", axis=0, tiled=True),
            lax.all_gather(blend_value_matrix.astype(jnp.bfloat16), "fs", axis=0, tiled=True),
        ),
    )
    conveyor_current = jax.nn.gelu(conveyor_prior * conveyor_rescalers)
    signal = jax.nn.gelu(stream_prior * blend_rescalers)
    total_sq = lax.psum(jnp.sum(signal * signal, axis=1), "tp")
    channels = signal.shape[1] * lax.axis_size("tp")
    signal_norm = (
        signal * lax.rsqrt(total_sq / channels + EPS)[:, None] * blend_norm_factor
    ).astype(jnp.bfloat16)
    local_groups = location_matrices.shape[0]
    block_len = location_matrices.shape[1]
    group_width = signal.shape[1] // local_groups
    lower_mask = jnp.tril(jnp.ones((block_len, block_len), bool))
    masked = jnp.where(lower_mask[None], location_matrices, jnp.zeros((), jnp.bfloat16))
    signal_blocks = signal_norm.reshape(-1, block_len, local_groups, group_width)
    location_blended = jnp.einsum(
        "gts,bsgd->btgd", masked, signal_blocks, preferred_element_type=jnp.float32
    )
    location_blended = location_blended + location_offsets.T[None, :, :, None]
    filtered_result = (conveyor_current * location_blended.reshape(conveyor_current.shape)).astype(
        jnp.bfloat16
    )
    mixer_terms = project_cols(
        filtered_result,
        out_scales,
        lax.all_gather(branch_emission_matrix.astype(jnp.bfloat16), "fs", axis=1, tiled=True),
    )
    summed = lax.psum(mixer_terms.astype(jnp.bfloat16), "tp").astype(jnp.float32)
    mid_rows = (full_rows.astype(jnp.float32) + summed).astype(jnp.bfloat16)
    mid_own = lax.dynamic_slice_in_dim(mid_rows, own_start, own_width, 1)
    ffn_in = normalize(mid_rows, latter_norm_factor)
    gate_half = valve_matrix.astype(jnp.bfloat16)
    up_half = raising_matrix.astype(jnp.bfloat16)
    whole_gate, whole_up = (
        lax.all_gather(gate_half, "fs", axis=0, tiled=True),
        lax.all_gather(up_half, "fs", axis=0, tiled=True),
    )
    pre_gate = jnp.dot(ffn_in, whole_gate, preferred_element_type=jnp.float32)
    pre_up = jnp.dot(ffn_in, whole_up, preferred_element_type=jnp.float32)
    hidden = (jax.nn.silu(pre_gate * valve_rescalers) * (pre_up * raising_rescalers)).astype(
        jnp.bfloat16
    )
    ffn_terms = project_cols(
        hidden,
        down_scales,
        lax.all_gather(lowering_matrix.astype(jnp.bfloat16), "fs", axis=1, tiled=True),
    )
    ffn_share = lax.psum_scatter(
        ffn_terms.astype(jnp.bfloat16), "tp", scatter_dimension=1, tiled=True
    ).astype(jnp.float32)
    return (mid_own.astype(jnp.float32) + ffn_share).astype(jnp.bfloat16)


def solution(mesh):
    sizes = dict(mesh.shape)
    fused = sizes["tp"] == 2 and sizes["fs"] == 16
    return jax.shard_map(
        on_device_fused if fused else on_device,
        mesh=mesh,
        in_specs=(
            P("fs", "tp"),
            P(),
            P("fs", "tp"),
            P("tp"),
            P("fs", "tp"),
            P("tp"),
            P("tp"),
            P("tp", None, None),
            P("tp", None),
            P("tp", "fs"),
            P("fs"),
            P(),
            P("fs", "tp"),
            P("tp"),
            P("fs", "tp"),
            P("tp"),
            P("tp", "fs"),
            P("fs"),
        ),
        out_specs=P("fs", "tp"),
        check_vma=False,
    )
```
